128 devices in a mesh: sp: 8 (over x, core), tp: 16 (over z, y).
Axes of the slice: x: 4, y: 4, z: 4, core: 2. Of those that a mesh axis runs over, the one named last changes fastest.
Arguments:
- tokens: bfloat16 [4, 2048, 2048], P(None, ('sp', 'tp')), may hold values from -6 to 6
- norm_gain: float32 [2048], replicated, may hold values from 0.5 to 1.5
- entry_projection: bfloat16 [2048, 2048], P(None, 'tp'), may hold values from -0.125 to 0.125
- valve_projection: bfloat16 [2048, 2048], P(None, 'tp'), may hold values from -0.125 to 0.125
- filter_taps: float32 [4, 2048], P(None, 'tp'), may hold values from -3 to 3
- conv_bias: float32 [2048], P('tp'), may hold values from -0.6 to 0.6
- recur_weight: bfloat16 [16, 128, 128], P('tp'), may hold values from -0.5 to 0.5
- recur_bias: float32 [2048], P('tp'), may hold values from -3 to 3
- entry_weight: bfloat16 [16, 128, 128], P('tp'), may hold values from -0.5 to 0.5
- entry_bias: float32 [2048], P('tp'), may hold values from -0.6 to 0.6
- forget_rate: float32 [2048], P('tp'), may hold values from 3.0517578e-05 to 0.25, as said below
- output_weight: bfloat16 [2048, 2048], P('tp'), may hold values from -0.5 to 0.5
Outputs:
- mixed: bfloat16 [4, 2048, 2048], P(None, ('sp', 'tp'))
The draws below stay inside these ranges and needn't reach their ends.
Inputs may be any that keep to these rules, and one draw needn't show every extreme that they name: forget_rate is positive; its even channels lie between 1 / 32768 and 1 / 8192, its odd channels between 1 / 64 and 1 / 4.
All inputs are finite; a program needn't handle non-finite values.
Results may differ from the reference program's by a relative error of at most 0.02.
Values may be sent and summed in bfloat16 or wider, within the bound.
A program may use at most 64 MiB of HBM per device.

```python
import jax
import jax.numpy as jnp
from jax import lax

D = 2048
D_LRU = 2048
BLOCKS = 16
WIDTH_BLOCK = 128
CONV_W = 4
SEQS = 4
SEQ_LEN = 2048


def draw_forget_rate(key, part):
    minimum_decay_bound = 1.0 / (16.0 * SEQ_LEN)
    slow_ceiling = 1.0 / (4.0 * SEQ_LEN)
    fast_floor = 1.0 / 64.0
    fast_ceiling = 0.25
    fractions = jax.random.uniform(key, (D_LRU,), jnp.float32)
    channel_index = jnp.arange(D_LRU)
    parity = (channel_index % 2).astype(jnp.float32)
    plain_floor = minimum_decay_bound + parity * (fast_floor - minimum_decay_bound)
    plain_ceiling = slow_ceiling + parity * (fast_ceiling - slow_ceiling)
    floor_log = jnp.log(plain_floor)
    ceiling_log = jnp.log(plain_ceiling)
    values = jnp.exp(floor_log + fractions * (ceiling_log - floor_log))
    values = jnp.clip(values, plain_floor, plain_ceiling)
    return values.astype(jnp.float32)


def levels(key, shape, split, low, largest):
    def one(position, shards_of):
        steps = jax.random.uniform(jax.random.fold_in(jax.random.fold_in(key, 6), position), (shards_of,), jnp.float32, low / len(split), largest / len(split))
        return jnp.repeat(jnp.exp(steps), shape[position] // shards_of).reshape((-1,) + (1,) * (len(shape) - position - 1))

    level = one(*split[0])
    for cut in split[1:]:
        level = level * one(*cut)
    return level


def centred(key, shape, width, reach, cuts=(), held_as=jnp.bfloat16):
    level = levels(key, shape, cuts, -0.22, 0.18) if cuts else 1.0
    drawn = jax.random.normal(key, shape, jnp.float32) * width * level
    return jnp.minimum(jnp.maximum(drawn, -reach), reach).astype(held_as)


def setup_inputs(seed: int = 0) -> dict:
    streams_of = jax.random.split(jax.random.key(seed), 13)
    tokens = centred(streams_of[0], (SEQS, SEQ_LEN, D), 1.0, 6.0, ((1, 128),))
    norm_gain = jnp.clip(1.0 + 0.1 * jax.random.normal(streams_of[1], (D,), jnp.float32), 0.5, 1.5)
    entry_projection = centred(streams_of[2], (D, D_LRU), D ** -0.5, 0.125, ((1, 16),))
    valve_projection = centred(streams_of[3], (D, D_LRU), D ** -0.5, 0.125, ((1, 16),))
    filter_taps = centred(streams_of[4], (CONV_W, D_LRU), 0.5, 3.0, ((1, 16),), jnp.float32)
    conv_bias = centred(streams_of[5], (D_LRU,), 0.1, 0.6, ((0, 16),), jnp.float32)
    recur_weight = centred(streams_of[6], (BLOCKS, WIDTH_BLOCK, WIDTH_BLOCK), WIDTH_BLOCK ** -0.5, 0.5, ((0, 16),))
    recur_bias = centred(streams_of[7], (D_LRU,), 0.5, 3.0, ((0, 16),), jnp.float32)
    entry_weight = centred(streams_of[8], (BLOCKS, WIDTH_BLOCK, WIDTH_BLOCK), WIDTH_BLOCK ** -0.5, 0.5, ((0, 16),))
    entry_bias = centred(streams_of[9], (D_LRU,), 0.1, 0.6, ((0, 16),), jnp.float32)
    forget_rate = draw_forget_rate(jax.random.fold_in(streams_of[12], 71), 0)
    output_weight = centred(streams_of[11], (D_LRU, D), (D_LRU // 16) ** -0.5, 0.5, ((0, 16),))
    return dict(tokens=tokens, norm_gain=norm_gain, entry_projection=entry_projection, valve_projection=valve_projection, filter_taps=filter_taps, conv_bias=conv_bias, recur_weight=recur_weight, recur_bias=recur_bias, entry_weight=entry_weight, entry_bias=entry_bias, forget_rate=forget_rate, output_weight=output_weight)


epsilon = 1e-06
gate_power = 8.0

def combine_pair(earlier, latter):
    return (earlier[0] * latter[0], latter[0] * earlier[1] + latter[1])

def block_product(convolved, weight):
    grouped = convolved.astype(jnp.float32).reshape(SEQ_LEN, BLOCKS, WIDTH_BLOCK)
    product = jnp.einsum('lhi,hij->lhj', grouped, weight.astype(jnp.float32), precision=lax.Precision.HIGHEST)
    return product.reshape(SEQ_LEN, D_LRU)

def reference(tokens, norm_gain, entry_projection, valve_projection, filter_taps, conv_bias, recur_weight, recur_bias, entry_weight, entry_bias, forget_rate, output_weight):

    def per_sequence(sequence):
        widened = sequence.astype(jnp.float32)
        scaled = widened * lax.rsqrt(lax.optimization_barrier(jnp.mean(widened * widened, axis=-1, keepdims=True)) + epsilon)
        rescaled_values = (scaled * norm_gain).astype(jnp.bfloat16)
        conv_input = jnp.dot(rescaled_values, entry_projection, preferred_element_type=jnp.float32).astype(jnp.bfloat16)
        gate_logits = jnp.dot(rescaled_values, valve_projection, preferred_element_type=jnp.float32).astype(jnp.bfloat16)
        padded = jnp.pad(conv_input, ((CONV_W - 1, 0), (0, 0))).astype(jnp.float32)
        summed = conv_bias + padded[0:SEQ_LEN] * filter_taps[0]
        for offset in range(1, CONV_W):
            summed = summed + padded[offset:offset + SEQ_LEN] * filter_taps[offset]
        convolved = summed.astype(jnp.bfloat16)
        recur_gate = jax.nn.sigmoid(block_product(convolved, recur_weight) + recur_bias)
        entry_gate = jax.nn.sigmoid(block_product(convolved, entry_weight) + entry_bias)
        log_decay = -gate_power * recur_gate * forget_rate
        decay = jnp.exp(log_decay)
        pushed = jnp.sqrt(-jnp.expm1(2.0 * log_decay)) * (entry_gate * convolved.astype(jnp.float32))
        hidden_state = lax.associative_scan(combine_pair, (decay, pushed), axis=0)[1]
        valved_lines = (hidden_state * jax.nn.silu(gate_logits.astype(jnp.float32))).astype(jnp.bfloat16)
        return jnp.dot(valved_lines, output_weight, preferred_element_type=jnp.float32).astype(jnp.bfloat16)
    return lax.map(per_sequence, tokens)
```

```python
import jax
import jax.numpy as jnp
from jax import lax
from jax.experimental import pallas as pl
from jax.experimental.pallas import tpu as pltpu
from jax.sharding import Mesh
from jax.sharding import PartitionSpec as P

MESH = pl.DeviceIdType.MESH
EPS = 1e-06
POWER = 8.0
SEQS = 4
TOK = 16
STR = 64
D = 2048
W = 128
NB = 4
CH = NB * W
ROWS = SEQS * STR
AROWS = D + 2 * W
PIECE = (AROWS // 8, D // 8, W // 8)
f32 = jnp.float32
bf16 = jnp.bfloat16


class Slots:
    def __init__(self):
        self.index = {}

    def __call__(self, *key):
        return self.index.setdefault(key, len(self.index))


N_COPIES = 104
N_LOCAL = 16


def neg_expm1(t):
    s = 1.0 + t * (1.0 / 8.0)
    for n in (7.0, 6.0, 5.0, 4.0, 3.0, 2.0):
        s = 1.0 + t * (1.0 / n) * s
    return jnp.where(t > -0.5, -t * s, 1.0 - jnp.exp(t))


def sigmoid(v):
    return 1.0 / (1.0 + jnp.exp(-v))


def kernel(
    tok_ref,
    gain_ref,
    w1_ref,
    w2_ref,
    rw_ref,
    ew_ref,
    small_ref,
    wo_ref,
    out_ref,
    tr,
    nt,
    wa,
    wv,
    wog,
    sm,
    ci,
    hs,
    hr,
    cv,
    lg,
    pc,
    hc,
    sg,
    gt,
    g16,
    s_own,
    l1,
    t_own,
    l2,
    pb,
    pf,
    rd,
    rb,
    ssem,
    rsem,
    lsem,
):
    X = lax.axis_index("x")
    C = lax.axis_index("c")
    Z = lax.axis_index("z")
    Y = lax.axis_index("y")
    g = X * 2 + C
    par = lax.rem(X, 2)

    def mod4(v):
        return lax.rem(v + 8, 4)

    def gdev(v):
        return {"x": v // 2, "c": lax.rem(v, 2)}

    nxt_z = mod4(Z + 1)
    nxt_g = lax.rem(g + jnp.where(Z == 3, 1, 0), 8)
    prv_z = mod4(Z - 1)
    prv_g = lax.rem(g + 8 - jnp.where(Z == 0, 1, 0), 8)
    nxt = {"x": nxt_g // 2, "c": lax.rem(nxt_g, 2), "z": nxt_z}
    prv = {"x": prv_g // 2, "c": lax.rem(prv_g, 2), "z": prv_z}
    yp, ym = {"y": mod4(Y + 1)}, {"y": mod4(Y - 1)}
    zp, zm = {"z": nxt_z}, {"z": prv_z}
    xp, xm = {"x": mod4(X + 1)}, {"x": mod4(X - 1)}
    mate = {"c": 1 - C}

    slot = Slots()
    local = Slots()
    sent = []

    def send(key, src, dst, dev):
        k = slot(*key)
        copy = pltpu.make_async_remote_copy(
            src_ref=src,
            dst_ref=dst,
            send_sem=ssem.at[k],
            recv_sem=rsem.at[k],
            device_id=dev,
            device_id_type=MESH,
        )
        copy.start()
        sent.append(copy)

    def arrived(key, dst):
        k = slot(*key)
        pltpu.make_async_remote_copy(
            src_ref=dst,
            dst_ref=dst,
            send_sem=ssem.at[k],
            recv_sem=rsem.at[k],
            device_id=mate,
            device_id_type=MESH,
        ).wait_recv()

    def fetch(key, src, dst):
        copy = pltpu.make_async_copy(src, dst, lsem.at[local(key)])
        copy.start()
        return copy

    lanes = pl.ds(pl.multiple_of(Z * W, W), W)
    own_tok = tr.at[:, pl.ds(pl.multiple_of(Y * TOK, TOK), TOK), :]
    c_tok = fetch("tok", tok_ref, own_tok)
    c_wa = [
        fetch("w1", w1_ref, wa.at[pl.ds(0, D), lanes]),
        fetch("rw", rw_ref.at[0], wa.at[pl.ds(D, W), lanes]),
        fetch("ew", ew_ref.at[0], wa.at[pl.ds(D + W, W), lanes]),
    ]
    c_sm = fetch("small", small_ref, sm.at[Z])
    c_wv = fetch("w2", w2_ref, wv.at[:, lanes])
    c_wo = fetch("wo", wo_ref, wog.at[pl.ds(pl.multiple_of(Z * W, W), W), :])

    l2[...] = jnp.zeros_like(l2)

    barrier = pltpu.get_barrier_semaphore()
    partners = [yp, ym] + [{"z": mod4(Z + d)} for d in (1, 2, 3)]
    partners += [gdev(lax.rem(g + d, 8)) for d in range(1, 8)] + [nxt, prv]
    for dev in partners:
        pl.semaphore_signal(barrier, inc=1, device_id=dev, device_id_type=MESH)
    pl.semaphore_wait(barrier, len(partners))

    def tok(y, half):
        return tr.at[pl.ds(2 * half, 2), pl.ds(pl.multiple_of(y * TOK, TOK), TOK), :]

    y_m, y_p, y_d = mod4(Y - 1), mod4(Y + 1), mod4(Y + 2)
    c_tok.wait()
    send(("t", 0, 0), tok(Y, 0), tok(Y, 0), yp)
    send(("t", 1, 1), tok(Y, 1), tok(Y, 1), ym)
    send(("t", 0, 1), tok(Y, 1), tok(Y, 1), yp)
    send(("t", 1, 0), tok(Y, 0), tok(Y, 0), ym)

    def piece(m, z, q, core, h):
        rows = PIECE[m]
        k = q * 4 + core * 2 + h
        if m == 2:
            return wog.at[pl.ds(pl.multiple_of(z * W + k * rows, rows), rows), :]
        ref = (wa, wv)[m]
        return ref.at[pl.ds(pl.multiple_of(k * rows, rows), rows), pl.ds(pl.multiple_of(z * W, W), W)]

    blocks = (mod4(Z - 1), mod4(Z + 1), mod4(Z + 2))

    def own_send(m):
        for j, h, dev in ((0, 0, zp), (1, 1, zm), (0, 1, zp), (1, 0, zm)):
            ref = piece(m, Z, par, C, h)
            send(("z", m, j, h), ref, ref, dev)

    def z_event(m, j, h):
        ref = piece(m, blocks[j], par, C, h)
        arrived(("z", m, j, h), ref)
        if (j, h) == (0, 0):
            send(("z", m, 2, 0), ref, ref, zp)
        if (j, h) == (1, 1):
            send(("z", m, 2, 1), ref, ref, zm)
        send(("x", m, j, h), ref, ref, xp if h == 0 else xm)
        send(("d", m, j, 0, h), ref, ref, mate)

    def x_event(m, j, h):
        ref = piece(m, blocks[j], 1 - par, C, h)
        arrived(("x", m, j, h), ref)
        send(("d", m, j, 1, h), ref, ref, mate)

    def d_events(m):
        for j in range(3):
            for src in range(2):
                for h in range(2):
                    q = par if src == 0 else 1 - par
                    arrived(("d", m, j, src, h), piece(m, blocks[j], q, 1 - C, h))

    for c in c_wa:
        c.wait()
    own_send(0)
    c_sm.wait()
    for d in (1, 2, 3):
        send(("s", d), sm.at[Z], sm.at[Z], {"z": mod4(Z + d)})

    def norm(y, half):
        rows = pl.ds(pl.multiple_of(y * TOK, TOK), TOK)
        v = tr[pl.ds(2 * half, 2), rows, :].astype(f32)
        v = v * lax.rsqrt(jnp.mean(v * v, axis=-1, keepdims=True) + EPS)
        v = (v * gain_ref[...].reshape(1, 1, D)).astype(bf16)
        for s in range(2):
            nt[pl.ds(pl.multiple_of((2 * half + s) * STR + y * TOK, TOK), TOK), :] = v[s]

    norm(Y, 0)
    norm(Y, 1)
    z_event(0, 0, 0)
    z_event(0, 1, 1)
    c_wv.wait()
    own_send(1)
    arrived(("t", 0, 0), tok(y_m, 0))
    send(("t", 2, 0), tok(y_m, 0), tok(y_m, 0), yp)
    arrived(("t", 1, 1), tok(y_p, 1))
    send(("t", 2, 1), tok(y_p, 1), tok(y_p, 1), ym)
    z_event(0, 0, 1)
    z_event(0, 1, 0)
    norm(y_m, 0)
    norm(y_p, 1)
    z_event(0, 2, 0)
    z_event(0, 2, 1)
    x_event(0, 0, 0)
    x_event(0, 1, 1)
    z_event(1, 0, 0)
    z_event(1, 1, 1)
    c_wo.wait()
    own_send(2)
    x_event(0, 0, 1)
    x_event(0, 1, 0)
    arrived(("t", 0, 1), tok(y_m, 1))
    norm(y_m, 1)
    arrived(("t", 1, 0), tok(y_p, 0))
    norm(y_p, 0)
    z_event(1, 0, 1)
    z_event(1, 1, 0)
    x_event(0, 2, 0)
    x_event(0, 2, 1)
    arrived(("t", 2, 0), tok(y_d, 0))
    norm(y_d, 0)
    arrived(("t", 2, 1), tok(y_d, 1))
    norm(y_d, 1)
    z_event(1, 2, 0)
    z_event(1, 2, 1)
    x_event(1, 0, 0)
    x_event(1, 1, 1)
    d_events(0)

    conv_in = jnp.dot(nt[...], wa[0:D, :], preferred_element_type=f32).astype(bf16)
    for b in range(NB):
        part = conv_in[:, b * W : (b + 1) * W]
        ci[b] = part.astype(f32)
        for s in range(SEQS):
            hs[b, s * 8 : s * 8 + 8, :] = ci[b, s * STR + STR - 8 : s * STR + STR, :]
    send(("h",), hs, hr, nxt)
    for d in (1, 2, 3):
        arrived(("s", d), sm.at[mod4(Z - d)])
    x_event(1, 0, 1)
    x_event(1, 1, 0)
    z_event(2, 0, 0)
    z_event(2, 1, 1)
    x_event(1, 2, 0)
    x_event(1, 2, 1)
    arrived(("h",), hr)

    lane_row = lax.broadcasted_iota(jnp.int32, (8, W), 0)
    first = jnp.where(jnp.logical_and(g == 0, Z == 0), 0.0, 1.0).astype(f32)
    for b in range(NB):
        taps = [sm[b, k] for k in range(4)]
        bias = sm[b, 4]
        for s in range(SEQS):
            x = [ci[b, pl.ds(s * STR + i, 8, stride=8), :] for i in range(8)]
            behind = hr[b, s * 8 : s * 8 + 8, :] * first
            prev = {}
            for i in (5, 6, 7):
                prev[i - 8] = jnp.where(
                    lane_row == 0,
                    jnp.broadcast_to(behind[i : i + 1, :], (8, W)),
                    pltpu.roll(x[i], 1, 0),
                )
            rows = []
            for i in range(8):
                acc = jnp.broadcast_to(bias, (8, W))
                for k in range(4):
                    src = i - 3 + k
                    acc = acc + (x[src] if src >= 0 else prev[src]) * taps[k]
                rows.append(acc)
            cv[pl.ds(s * STR, STR), b * W : (b + 1) * W] = jnp.concatenate(rows, axis=0).astype(bf16)

    ends_a = [[None] * SEQS for _ in range(NB)]
    for b in range(NB):
        cols = slice(b * W, (b + 1) * W)
        block = cv[:, cols]
        lg[0] = jnp.dot(block, wa[D : D + W, cols], preferred_element_type=f32)
        lg[1] = jnp.dot(block, wa[D + W : D + 2 * W, cols], preferred_element_type=f32)
        r_bias, e_bias, rate = sm[b, 5], sm[b, 6], sm[b, 7]
        for s in range(SEQS):
            rows = slice(s * STR, (s + 1) * STR)
            r_gate = sigmoid(lg[0, rows, :] + r_bias)
            e_gate = sigmoid(lg[1, rows, :] + e_bias)
            log_decay = (-POWER * r_gate) * rate
            decay = jnp.exp(log_decay)
            pushed = jnp.sqrt(neg_expm1(2.0 * log_decay)) * (e_gate * cv[rows, cols].astype(f32))
            a = decay[0:8]
            h = pushed[0:8]
            pc[b, s * STR : s * STR + 8, :] = a
            hc[b, s * STR : s * STR + 8, :] = h
            for i in range(1, 8):
                step = decay[i * 8 : i * 8 + 8]
                h = step * h + pushed[i * 8 : i * 8 + 8]
                a = step * a
                pc[b, s * STR + i * 8 : s * STR + i * 8 + 8, :] = a
                hc[b, s * STR + i * 8 : s * STR + i * 8 + 8, :] = h
            for n in (1, 2, 4):
                keep = lane_row >= n
                a_in = jnp.where(keep, pltpu.roll(a, n, 0), 1.0)
                h_in = jnp.where(keep, pltpu.roll(h, n, 0), 0.0)
                h = a * h_in + h
                a = a * a_in
            s_own[s : s + 1, cols] = a[7:8]
            s_own[4 + s : 5 + s, cols] = h[7:8]
            ends_a[b][s] = (
                jnp.where(lane_row >= 1, pltpu.roll(a, 1, 0), 1.0),
                jnp.where(lane_row >= 1, pltpu.roll(h, 1, 0), 0.0),
            )

    for d in (1, 2, 3):
        send(("e", d), s_own, l1.at[Z], {"z": mod4(Z + d)})
    l1[Z] = s_own[...]
    z_event(2, 0, 1)
    z_event(2, 1, 0)
    x_event(2, 0, 0)
    x_event(2, 1, 1)
    for d in (1, 2, 3):
        arrived(("e", d), l1.at[mod4(Z - d)])
    total_a, total_h = l1[0, 0:4], l1[0, 4:8]
    for k in range(1, 4):
        ka, kh = l1[k, 0:4], l1[k, 4:8]
        total_h = ka * total_h + kh
        total_a = ka * total_a
    t_own[0:4] = total_a
    t_own[4:8] = total_h
    for d in range(1, 8):
        k = slot("g", d)

        @pl.when(g + d < 8)
        def _():
            pltpu.make_async_remote_copy(
                src_ref=t_own,
                dst_ref=l2.at[g],
                send_sem=ssem.at[k],
                recv_sem=rsem.at[k],
                device_id=gdev(lax.rem(g + d, 8)),
                device_id_type=MESH,
            ).start()

    z_event(2, 2, 0)
    z_event(2, 2, 1)
    d_events(1)
    x_event(2, 0, 1)
    x_event(2, 1, 0)
    logits = jnp.dot(nt[...], wv[...], preferred_element_type=f32).astype(bf16).astype(f32)
    for b in range(NB):
        v = logits[:, b * W : (b + 1) * W]
        sg[b] = v / (1.0 + jnp.exp(-v))
    x_event(2, 2, 0)
    x_event(2, 2, 1)
    for d in range(1, 8):
        k = slot("g", d)

        @pl.when(g - d >= 0)
        def _():
            ref = l2.at[lax.rem(g - d + 8, 8)]
            pltpu.make_async_remote_copy(
                src_ref=ref,
                dst_ref=ref,
                send_sem=ssem.at[k],
                recv_sem=rsem.at[k],
                device_id=mate,
                device_id_type=MESH,
            ).wait_recv()

    state = jnp.zeros((SEQS, CH), f32)
    for k in range(7):
        state = jnp.where(k < g, l2[k, 0:4] * state + l2[k, 4:8], state)
    for k in range(3):
        state = jnp.where(k < Z, l1[k, 0:4] * state + l1[k, 4:8], state)

    for b in range(NB):
        cols = slice(b * W, (b + 1) * W)
        for s in range(SEQS):
            chain_a, chain_h = ends_a[b][s]
            enter = chain_a * jnp.broadcast_to(state[s : s + 1, cols], (8, W)) + chain_h
            for i in range(8):
                at = s * STR + i * 8
                h = pc[b, at : at + 8, :] * enter + hc[b, at : at + 8, :]
                places = pl.ds(s * STR + i, 8, stride=8)
                gt[b, places, :] = h * sg[b, places, :]
        g16[:, cols] = gt[b].astype(bf16)

    d_events(2)

    def product(y):
        lhs = jnp.concatenate(
            [g16[pl.ds(pl.multiple_of(s * STR + y * TOK, TOK), TOK), :] for s in range(SEQS)], axis=0
        )
        return jnp.dot(lhs, wog[...], preferred_element_type=f32)

    p = product(y_d).astype(bf16).reshape(SEQS, TOK, D)
    pb[0] = p
    send(("r", 0), pb.at[0, pl.ds(0, 2)], rd.at[0], ym)
    send(("r", 1), pb.at[0, pl.ds(2, 2)], rd.at[1], yp)
    p = product(y_p).reshape(SEQS, TOK, D)
    pb[1, 0:2] = p[0:2].astype(bf16)
    send(("r", 2), pb.at[1, pl.ds(0, 2)], rb.at[0, pl.ds(0, 2)], yp)
    pf[1] = p[2:4]
    p = product(y_m).reshape(SEQS, TOK, D)
    pb[2, 2:4] = p[2:4].astype(bf16)
    send(("r", 3), pb.at[2, pl.ds(2, 2)], rb.at[1, pl.ds(2, 2)], ym)
    pf[0] = p[0:2]
    mine = product(Y).reshape(SEQS, TOK, D)
    arrived(("r", 1), rd.at[1])
    pb[1, 2:4] = (pf[1] + rd[1].astype(f32)).astype(bf16)
    send(("r", 4), pb.at[1, pl.ds(2, 2)], rb.at[0, pl.ds(2, 2)], yp)
    arrived(("r", 0), rd.at[0])
    pb[2, 0:2] = (pf[0] + rd[0].astype(f32)).astype(bf16)
    send(("r", 5), pb.at[2, pl.ds(0, 2)], rb.at[1, pl.ds(0, 2)], ym)
    arrived(("r", 2), rb.at[0, pl.ds(0, 2)])
    arrived(("r", 3), rb.at[1, pl.ds(2, 2)])
    arrived(("r", 4), rb.at[0, pl.ds(2, 2)])
    arrived(("r", 5), rb.at[1, pl.ds(0, 2)])
    out_ref[...] = (mine + rb[0].astype(f32) + rb[1].astype(f32)).astype(bf16)

    for copy in sent:
        copy.wait_send()
    for d in range(1, 8):
        k = slot("g", d)

        @pl.when(g + d < 8)
        def _():
            pltpu.make_async_remote_copy(
                src_ref=t_own,
                dst_ref=l2.at[g],
                send_sem=ssem.at[k],
                recv_sem=rsem.at[k],
                device_id=gdev(lax.rem(g + d, 8)),
                device_id_type=MESH,
            ).wait_send()


def per_device(
    tokens,
    norm_gain,
    entry_projection,
    valve_projection,
    filter_taps,
    conv_bias,
    recur_weight,
    recur_bias,
    entry_weight,
    entry_bias,
    forget_rate,
    output_weight,
):
    small = jnp.concatenate(
        [filter_taps, conv_bias[None], recur_bias[None], entry_bias[None], forget_rate[None]], axis=0
    ).reshape(8, 1, W)
    anywhere = pl.BlockSpec(memory_space=pl.ANY)
    vmem = pl.BlockSpec(memory_space=pltpu.VMEM)
    return pl.pallas_call(
        kernel,
        name="layer",
        out_shape=jax.ShapeDtypeStruct((SEQS, TOK, D), bf16),
        in_specs=[anywhere, vmem, anywhere, anywhere, anywhere, anywhere, anywhere, anywhere],
        out_specs=vmem,
        scratch_shapes=[
            pltpu.VMEM((SEQS, STR, D), bf16),
            pltpu.VMEM((ROWS, D), bf16),
            pltpu.VMEM((AROWS, CH), bf16),
            pltpu.VMEM((D, CH), bf16),
            pltpu.VMEM((CH, D), bf16),
            pltpu.VMEM((NB, 8, 1, W), f32),
            pltpu.VMEM((NB, ROWS, W), f32),
            pltpu.VMEM((NB, 32, W), f32),
            pltpu.VMEM((NB, 32, W), f32),
            pltpu.VMEM((ROWS, CH), bf16),
            pltpu.VMEM((2, ROWS, W), f32),
            pltpu.VMEM((NB, ROWS, W), f32),
            pltpu.VMEM((NB, ROWS, W), f32),
            pltpu.VMEM((NB, ROWS, W), f32),
            pltpu.VMEM((NB, ROWS, W), f32),
            pltpu.VMEM((ROWS, CH), bf16),
            pltpu.VMEM((8, CH), f32),
            pltpu.VMEM((4, 8, CH), f32),
            pltpu.VMEM((8, CH), f32),
            pltpu.VMEM((8, 8, CH), f32),
            pltpu.VMEM((3, SEQS, TOK, D), bf16),
            pltpu.VMEM((2, 2, TOK, D), f32),
            pltpu.VMEM((2, 2, TOK, D), bf16),
            pltpu.VMEM((2, SEQS, TOK, D), bf16),
            pltpu.SemaphoreType.DMA((N_COPIES,)),
            pltpu.SemaphoreType.DMA((N_COPIES,)),
            pltpu.SemaphoreType.DMA((N_LOCAL,)),
        ],
        compiler_params=pltpu.CompilerParams(
            collective_id=0, has_side_effects=True, vmem_limit_bytes=48 * 1024 * 1024
        ),
    )(
        tokens,
        norm_gain.reshape(1, D),
        entry_projection,
        valve_projection,
        recur_weight,
        entry_weight,
        small,
        output_weight,
    )


def solution(mesh):
    fine = Mesh(mesh.devices.reshape(4, 2, 4, 4), ("x", "c", "z", "y"))
    SP, TP = ("x", "c"), ("z", "y")
    both = SP + TP
    placed = (
        P(None, both, None),
        P(),
        P(None, TP),
        P(None, TP),
        P(None, TP),
        P(TP),
        P(TP, None, None),
        P(TP),
        P(TP, None, None),
        P(TP),
        P(TP),
        P(TP, None),
    )
    return jax.shard_map(
        per_device, mesh=fine, in_specs=placed, out_specs=P(None, both, None), check_vma=False
    )
```

```python
import jax
import jax.numpy as jnp
from jax import lax
from jax.experimental import pallas as pl
from jax.experimental.pallas import tpu as pltpu
from jax.sharding import Mesh
from jax.sharding import PartitionSpec as P

MESH = pl.DeviceIdType.MESH
EPS = 1e-06
POWER = 8.0
SEQS = 4
TOK = 16
STR = 64
D = 2048
W = 128
NB = 4
CH = NB * W
ROWS = SEQS * STR
AROWS = D + 2 * W
PIECE = (AROWS // 8, D // 8, W // 8)
f32 = jnp.float32
bf16 = jnp.bfloat16


class Slots:
    def __init__(self):
        self.index = {}

    def __call__(self, *key):
        return self.index.setdefault(key, len(self.index))


N_COPIES = 104
N_LOCAL = 16
VMEM_LIMIT = 67043328


def neg_expm1(t):
    s = 1.0 + t * (1.0 / 8.0)
    for n in (7.0, 6.0, 5.0, 4.0, 3.0, 2.0):
        s = 1.0 + t * (1.0 / n) * s
    return jnp.where(t > -0.5, -t * s, 1.0 - jnp.exp(t))


def sigmoid(v):
    return 1.0 / (1.0 + jnp.exp(-v))


def kernel(
    tok_ref,
    gain_ref,
    w1_ref,
    w2_ref,
    rw_ref,
    ew_ref,
    taps_ref,
    cb_ref,
    rb_ref,
    eb_ref,
    rate_ref,
    wo_ref,
    out_ref,
    gain,
    tr,
    nt,
    wa,
    wv,
    wog,
    sm,
    ci,
    hs,
    hr,
    cv,
    lg,
    pc,
    hc,
    sg,
    gt,
    g16,
    s_own,
    l1,
    t_own,
    l2,
    pb,
    pf,
    rd,
    rb,
    ssem,
    rsem,
    lsem,
):
    X = lax.axis_index("x")
    C = lax.axis_index("c")
    Z = lax.axis_index("z")
    Y = lax.axis_index("y")
    g = X * 2 + C
    par = lax.rem(X, 2)

    def mod4(v):
        return lax.rem(v + 8, 4)

    def gdev(v):
        return {"x": v // 2, "c": lax.rem(v, 2)}

    nxt_z = mod4(Z + 1)
    nxt_g = lax.rem(g + jnp.where(Z == 3, 1, 0), 8)
    prv_z = mod4(Z - 1)
    prv_g = lax.rem(g + 8 - jnp.where(Z == 0, 1, 0), 8)
    nxt = {"x": nxt_g // 2, "c": lax.rem(nxt_g, 2), "z": nxt_z}
    prv = {"x": prv_g // 2, "c": lax.rem(prv_g, 2), "z": prv_z}
    yp, ym = {"y": mod4(Y + 1)}, {"y": mod4(Y - 1)}
    zp, zm = {"z": nxt_z}, {"z": prv_z}
    xp, xm = {"x": mod4(X + 1)}, {"x": mod4(X - 1)}
    mate = {"c": 1 - C}

    slot = Slots()
    local = Slots()
    sent = []
    scopes = []

    def mark(name):
        if scopes:
            scopes.pop().__exit__(None, None, None)
        if name:
            scopes.append(jax.named_scope(name))
            scopes[-1].__enter__()

    def send(key, src, dst, dev):
        k = slot(*key)
        copy = pltpu.make_async_remote_copy(
            src_ref=src,
            dst_ref=dst,
            send_sem=ssem.at[k],
            recv_sem=rsem.at[k],
            device_id=dev,
            device_id_type=MESH,
        )
        copy.start()
        sent.append(copy)

    def arrived(key, dst):
        k = slot(*key)
        pltpu.make_async_remote_copy(
            src_ref=dst,
            dst_ref=dst,
            send_sem=ssem.at[k],
            recv_sem=rsem.at[k],
            device_id=mate,
            device_id_type=MESH,
        ).wait_recv()

    def fetch(key, src, dst):
        copy = pltpu.make_async_copy(src, dst, lsem.at[local(key)])
        copy.start()
        return copy

    mark("own")
    lanes = pl.ds(pl.multiple_of(Z * W, W), W)
    own_tok = tr.at[:, pl.ds(pl.multiple_of(Y * TOK, TOK), TOK), :]
    c_tok = fetch("tok", tok_ref, own_tok)
    c_wa = [
        fetch("w1", w1_ref, wa.at[pl.ds(0, D), lanes]),
        fetch("rw", rw_ref.at[0], wa.at[pl.ds(D, W), lanes]),
        fetch("ew", ew_ref.at[0], wa.at[pl.ds(D + W, W), lanes]),
    ]
    c_sm = [fetch("taps", taps_ref, sm.at[Z, pl.ds(0, 4)])]
    for n, ref in enumerate((cb_ref, rb_ref, eb_ref, rate_ref)):
        c_sm.append(fetch(("row", n), ref, sm.at[Z, 4 + n]))
    c_gain = fetch("gain", gain_ref, gain)
    c_wv = fetch("w2", w2_ref, wv.at[:, lanes])
    c_wo = fetch("wo", wo_ref, wog.at[pl.ds(pl.multiple_of(Z * W, W), W), :])

    l2[...] = jnp.zeros_like(l2)

    mark("barrier")
    barrier = pltpu.get_barrier_semaphore()
    partners = [yp, ym] + [{"z": mod4(Z + d)} for d in (1, 2, 3)]
    partners += [gdev(lax.rem(g + d, 8)) for d in range(1, 8)] + [nxt, prv]
    for dev in partners:
        pl.semaphore_signal(barrier, inc=1, device_id=dev, device_id_type=MESH)
    pl.semaphore_wait(barrier, len(partners))

    mark("tokens")
    def tok(y, half):
        return tr.at[pl.ds(2 * half, 2), pl.ds(pl.multiple_of(y * TOK, TOK), TOK), :]

    y_m, y_p, y_d = mod4(Y - 1), mod4(Y + 1), mod4(Y + 2)
    c_tok.wait()
    send(("t", 0, 0), tok(Y, 0), tok(Y, 0), yp)
    send(("t", 1, 1), tok(Y, 1), tok(Y, 1), ym)
    send(("t", 0, 1), tok(Y, 1), tok(Y, 1), yp)
    send(("t", 1, 0), tok(Y, 0), tok(Y, 0), ym)

    def piece(m, z, q, core, h):
        rows = PIECE[m]
        k = q * 4 + core * 2 + h
        if m == 2:
            return wog.at[pl.ds(pl.multiple_of(z * W + k * rows, rows), rows), :]
        ref = (wa, wv)[m]
        return ref.at[pl.ds(pl.multiple_of(k * rows, rows), rows), pl.ds(pl.multiple_of(z * W, W), W)]

    blocks = (mod4(Z - 1), mod4(Z + 1), mod4(Z + 2))

    def own_send(m):
        for j, h, dev in ((0, 0, zp), (1, 1, zm), (0, 1, zp), (1, 0, zm)):
            ref = piece(m, Z, par, C, h)
            send(("z", m, j, h), ref, ref, dev)

    def z_event(m, j, h):
        ref = piece(m, blocks[j], par, C, h)
        arrived(("z", m, j, h), ref)
        if (j, h) == (0, 0):
            send(("z", m, 2, 0), ref, ref, zp)
        if (j, h) == (1, 1):
            send(("z", m, 2, 1), ref, ref, zm)
        send(("x", m, j, h), ref, ref, xp if h == 0 else xm)
        send(("d", m, j, 0, h), ref, ref, mate)

    def x_event(m, j, h):
        ref = piece(m, blocks[j], 1 - par, C, h)
        arrived(("x", m, j, h), ref)
        send(("d", m, j, 1, h), ref, ref, mate)

    def d_events(m):
        for j in range(3):
            for src in range(2):
                for h in range(2):
                    q = par if src == 0 else 1 - par
                    arrived(("d", m, j, src, h), piece(m, blocks[j], q, 1 - C, h))

    mark("weights")
    for c in c_wa:
        c.wait()
    own_send(0)
    for c in c_sm:
        c.wait()
    for d in (1, 2, 3):
        send(("s", d), sm.at[Z], sm.at[Z], {"z": mod4(Z + d)})

    def norm(y, half):
        rows = pl.ds(pl.multiple_of(y * TOK, TOK), TOK)
        v = tr[pl.ds(2 * half, 2), rows, :].astype(f32)
        v = v * lax.rsqrt(jnp.mean(v * v, axis=-1, keepdims=True) + EPS)
        v = (v * gain[...].reshape(1, 1, D)).astype(bf16)
        for s in range(2):
            nt[pl.ds(pl.multiple_of((2 * half + s) * STR + y * TOK, TOK), TOK), :] = v[s]

    mark("norm0")
    c_gain.wait()
    norm(Y, 0)
    norm(Y, 1)
    mark("net0")
    z_event(0, 0, 0)
    z_event(0, 1, 1)
    c_wv.wait()
    own_send(1)
    arrived(("t", 0, 0), tok(y_m, 0))
    send(("t", 2, 0), tok(y_m, 0), tok(y_m, 0), yp)
    arrived(("t", 1, 1), tok(y_p, 1))
    send(("t", 2, 1), tok(y_p, 1), tok(y_p, 1), ym)
    mark("net1")
    z_event(0, 0, 1)
    z_event(0, 1, 0)
    mark("norm1")
    norm(y_m, 0)
    norm(y_p, 1)
    mark("net2")
    z_event(0, 2, 0)
    z_event(0, 2, 1)
    x_event(0, 0, 0)
    x_event(0, 1, 1)
    z_event(1, 0, 0)
    z_event(1, 1, 1)
    c_wo.wait()
    own_send(2)
    mark("net3")
    x_event(0, 0, 1)
    x_event(0, 1, 0)
    mark("norm2")
    arrived(("t", 0, 1), tok(y_m, 1))
    norm(y_m, 1)
    arrived(("t", 1, 0), tok(y_p, 0))
    norm(y_p, 0)
    mark("net4")
    z_event(1, 0, 1)
    z_event(1, 1, 0)
    x_event(0, 2, 0)
    x_event(0, 2, 1)
    mark("norm3")
    arrived(("t", 2, 0), tok(y_d, 0))
    norm(y_d, 0)
    arrived(("t", 2, 1), tok(y_d, 1))
    norm(y_d, 1)
    mark("net5")
    z_event(1, 2, 0)
    z_event(1, 2, 1)
    x_event(1, 0, 0)
    x_event(1, 1, 1)
    mark("d0")
    d_events(0)

    mark("matmul1")
    conv_in = jnp.dot(nt[...], wa[0:D, :], preferred_element_type=f32).astype(bf16)
    for b in range(NB):
        part = conv_in[:, b * W : (b + 1) * W]
        ci[b] = part.astype(f32)
        for s in range(SEQS):
            hs[b, s * 8 : s * 8 + 8, :] = ci[b, s * STR + STR - 8 : s * STR + STR, :]
    send(("h",), hs, hr, nxt)
    mark("net6")
    for d in (1, 2, 3):
        arrived(("s", d), sm.at[mod4(Z - d)])
    x_event(1, 0, 1)
    x_event(1, 1, 0)
    z_event(2, 0, 0)
    z_event(2, 1, 1)
    x_event(1, 2, 0)
    x_event(1, 2, 1)
    mark("halo")
    arrived(("h",), hr)

    mark("conv")
    lane_row = lax.broadcasted_iota(jnp.int32, (8, W), 0)
    first = jnp.where(jnp.logical_and(g == 0, Z == 0), 0.0, 1.0).astype(f32)
    for b in range(NB):
        taps = [sm[b, k] for k in range(4)]
        bias = sm[b, 4]
        for s in range(SEQS):
            x = [ci[b, pl.ds(s * STR + i, 8, stride=8), :] for i in range(8)]
            behind = hr[b, s * 8 : s * 8 + 8, :] * first
            prev = {}
            for i in (5, 6, 7):
                prev[i - 8] = jnp.where(
                    lane_row == 0,
                    jnp.broadcast_to(behind[i : i + 1, :], (8, W)),
                    pltpu.roll(x[i], 1, 0),
                )
            rows = []
            for i in range(8):
                acc = jnp.broadcast_to(bias, (8, W))
                for k in range(4):
                    src = i - 3 + k
                    acc = acc + (x[src] if src >= 0 else prev[src]) * taps[k]
                rows.append(acc)
            cv[pl.ds(s * STR, STR), b * W : (b + 1) * W] = jnp.concatenate(rows, axis=0).astype(bf16)

    mark("gates")
    ends_a = [[None] * SEQS for _ in range(NB)]
    for b in range(NB):
        cols = slice(b * W, (b + 1) * W)
        block = cv[:, cols]
        lg[0] = jnp.dot(block, wa[D : D + W, cols], preferred_element_type=f32)
        lg[1] = jnp.dot(block, wa[D + W : D + 2 * W, cols], preferred_element_type=f32)
        r_bias, e_bias, rate = sm[b, 5], sm[b, 6], sm[b, 7]
        for s in range(SEQS):
            rows = slice(s * STR, (s + 1) * STR)
            r_gate = sigmoid(lg[0, rows, :] + r_bias)
            e_gate = sigmoid(lg[1, rows, :] + e_bias)
            log_decay = (-POWER * r_gate) * rate
            decay = jnp.exp(log_decay)
            pushed = jnp.sqrt(neg_expm1(2.0 * log_decay)) * (e_gate * cv[rows, cols].astype(f32))
            a = decay[0:8]
            h = pushed[0:8]
            pc[b, s * STR : s * STR + 8, :] = a
            hc[b, s * STR : s * STR + 8, :] = h
            for i in range(1, 8):
                step = decay[i * 8 : i * 8 + 8]
                h = step * h + pushed[i * 8 : i * 8 + 8]
                a = step * a
                pc[b, s * STR + i * 8 : s * STR + i * 8 + 8, :] = a
                hc[b, s * STR + i * 8 : s * STR + i * 8 + 8, :] = h
            for n in (1, 2, 4):
                keep = lane_row >= n
                a_in = jnp.where(keep, pltpu.roll(a, n, 0), 1.0)
                h_in = jnp.where(keep, pltpu.roll(h, n, 0), 0.0)
                h = a * h_in + h
                a = a * a_in
            s_own[s : s + 1, cols] = a[7:8]
            s_own[4 + s : 5 + s, cols] = h[7:8]
            ends_a[b][s] = (
                jnp.where(lane_row >= 1, pltpu.roll(a, 1, 0), 1.0),
                jnp.where(lane_row >= 1, pltpu.roll(h, 1, 0), 0.0),
            )

    mark("states")
    for d in (1, 2, 3):
        send(("e", d), s_own, l1.at[Z], {"z": mod4(Z + d)})
    l1[Z] = s_own[...]
    z_event(2, 0, 1)
    z_event(2, 1, 0)
    x_event(2, 0, 0)
    x_event(2, 1, 1)
    mark("states1")
    for d in (1, 2, 3):
        arrived(("e", d), l1.at[mod4(Z - d)])
    total_a, total_h = l1[0, 0:4], l1[0, 4:8]
    for k in range(1, 4):
        ka, kh = l1[k, 0:4], l1[k, 4:8]
        total_h = ka * total_h + kh
        total_a = ka * total_a
    t_own[0:4] = total_a
    t_own[4:8] = total_h
    for d in range(1, 8):
        k = slot("g", d)

        @pl.when(g + d < 8)
        def _():
            pltpu.make_async_remote_copy(
                src_ref=t_own,
                dst_ref=l2.at[g],
                send_sem=ssem.at[k],
                recv_sem=rsem.at[k],
                device_id=gdev(lax.rem(g + d, 8)),
                device_id_type=MESH,
            ).start()

    mark("net8")
    z_event(2, 2, 0)
    z_event(2, 2, 1)
    d_events(1)
    x_event(2, 0, 1)
    x_event(2, 1, 0)
    mark("valve")
    logits = jnp.dot(nt[...], wv[...], preferred_element_type=f32).astype(bf16).astype(f32)
    for b in range(NB):
        v = logits[:, b * W : (b + 1) * W]
        sg[b] = v / (1.0 + jnp.exp(-v))
    mark("states2")
    x_event(2, 2, 0)
    x_event(2, 2, 1)
    for d in range(1, 8):
        k = slot("g", d)

        @pl.when(g - d >= 0)
        def _():
            ref = l2.at[lax.rem(g - d + 8, 8)]
            pltpu.make_async_remote_copy(
                src_ref=ref,
                dst_ref=ref,
                send_sem=ssem.at[k],
                recv_sem=rsem.at[k],
                device_id=mate,
                device_id_type=MESH,
            ).wait_recv()

    mark("entering")
    state = jnp.zeros((SEQS, CH), f32)
    for k in range(7):
        state = jnp.where(k < g, l2[k, 0:4] * state + l2[k, 4:8], state)
    for k in range(3):
        state = jnp.where(k < Z, l1[k, 0:4] * state + l1[k, 4:8], state)

    mark("gated")
    for b in range(NB):
        cols = slice(b * W, (b + 1) * W)
        for s in range(SEQS):
            chain_a, chain_h = ends_a[b][s]
            enter = chain_a * jnp.broadcast_to(state[s : s + 1, cols], (8, W)) + chain_h
            for i in range(8):
                at = s * STR + i * 8
                h = pc[b, at : at + 8, :] * enter + hc[b, at : at + 8, :]
                places = pl.ds(s * STR + i, 8, stride=8)
                gt[b, places, :] = h * sg[b, places, :]
        g16[:, cols] = gt[b].astype(bf16)

    mark("d2")
    d_events(2)

    def product(y):
        lhs = jnp.concatenate(
            [g16[pl.ds(pl.multiple_of(s * STR + y * TOK, TOK), TOK), :] for s in range(SEQS)], axis=0
        )
        return jnp.dot(lhs, wog[...], preferred_element_type=f32)

    mark("prod0")
    p = product(y_d).astype(bf16).reshape(SEQS, TOK, D)
    pb[0] = p
    send(("r", 0), pb.at[0, pl.ds(0, 2)], rd.at[0], ym)
    send(("r", 1), pb.at[0, pl.ds(2, 2)], rd.at[1], yp)
    mark("prod1")
    p = product(y_p).reshape(SEQS, TOK, D)
    pb[1, 0:2] = p[0:2].astype(bf16)
    send(("r", 2), pb.at[1, pl.ds(0, 2)], rb.at[0, pl.ds(0, 2)], yp)
    pf[1] = p[2:4]
    p = product(y_m).reshape(SEQS, TOK, D)
    pb[2, 2:4] = p[2:4].astype(bf16)
    send(("r", 3), pb.at[2, pl.ds(2, 2)], rb.at[1, pl.ds(2, 2)], ym)
    pf[0] = p[0:2]
    mine = product(Y).reshape(SEQS, TOK, D)
    mark("red1")
    arrived(("r", 1), rd.at[1])
    pb[1, 2:4] = (pf[1] + rd[1].astype(f32)).astype(bf16)
    send(("r", 4), pb.at[1, pl.ds(2, 2)], rb.at[0, pl.ds(2, 2)], yp)
    arrived(("r", 0), rd.at[0])
    pb[2, 0:2] = (pf[0] + rd[0].astype(f32)).astype(bf16)
    send(("r", 5), pb.at[2, pl.ds(0, 2)], rb.at[1, pl.ds(0, 2)], ym)
    mark("red2")
    arrived(("r", 2), rb.at[0, pl.ds(0, 2)])
    arrived(("r", 3), rb.at[1, pl.ds(2, 2)])
    arrived(("r", 4), rb.at[0, pl.ds(2, 2)])
    arrived(("r", 5), rb.at[1, pl.ds(0, 2)])
    mark("final")
    out_ref[...] = (mine + rb[0].astype(f32) + rb[1].astype(f32)).astype(bf16)

    mark("drain")
    for copy in sent:
        copy.wait_send()
    for d in range(1, 8):
        k = slot("g", d)

        @pl.when(g + d < 8)
        def _():
            pltpu.make_async_remote_copy(
                src_ref=t_own,
                dst_ref=l2.at[g],
                send_sem=ssem.at[k],
                recv_sem=rsem.at[k],
                device_id=gdev(lax.rem(g + d, 8)),
                device_id_type=MESH,
            ).wait_send()

    mark(None)


def per_device(
    tokens,
    norm_gain,
    entry_projection,
    valve_projection,
    filter_taps,
    conv_bias,
    recur_weight,
    recur_bias,
    entry_weight,
    entry_bias,
    forget_rate,
    output_weight,
):
    hbm = pl.BlockSpec(memory_space=pltpu.HBM)
    vmem = pl.BlockSpec(memory_space=pltpu.VMEM)
    return pl.pallas_call(
        kernel,
        name="layer",
        out_shape=jax.ShapeDtypeStruct((SEQS, TOK, D), bf16),
        in_specs=[hbm] * 12,
        out_specs=vmem,
        scratch_shapes=[
            pltpu.VMEM((1, D), f32),
            pltpu.VMEM((SEQS, STR, D), bf16),
            pltpu.VMEM((ROWS, D), bf16),
            pltpu.VMEM((AROWS, CH), bf16),
            pltpu.VMEM((D, CH), bf16),
            pltpu.VMEM((CH, D), bf16),
            pltpu.VMEM((NB, 8, 1, W), f32),
            pltpu.VMEM((NB, ROWS, W), f32),
            pltpu.VMEM((NB, 32, W), f32),
            pltpu.VMEM((NB, 32, W), f32),
            pltpu.VMEM((ROWS, CH), bf16),
            pltpu.VMEM((2, ROWS, W), f32),
            pltpu.VMEM((NB, ROWS, W), f32),
            pltpu.VMEM((NB, ROWS, W), f32),
            pltpu.VMEM((NB, ROWS, W), f32),
            pltpu.VMEM((NB, ROWS, W), f32),
            pltpu.VMEM((ROWS, CH), bf16),
            pltpu.VMEM((8, CH), f32),
            pltpu.VMEM((4, 8, CH), f32),
            pltpu.VMEM((8, CH), f32),
            pltpu.VMEM((8, 8, CH), f32),
            pltpu.VMEM((3, SEQS, TOK, D), bf16),
            pltpu.VMEM((2, 2, TOK, D), f32),
            pltpu.VMEM((2, 2, TOK, D), bf16),
            pltpu.VMEM((2, SEQS, TOK, D), bf16),
            pltpu.SemaphoreType.DMA((N_COPIES,)),
            pltpu.SemaphoreType.DMA((N_COPIES,)),
            pltpu.SemaphoreType.DMA((N_LOCAL,)),
        ],
        compiler_params=pltpu.CompilerParams(
            collective_id=0, has_side_effects=True, vmem_limit_bytes=VMEM_LIMIT
        ),
    )(
        tokens,
        norm_gain.reshape(1, D),
        entry_projection,
        valve_projection,
        recur_weight,
        entry_weight,
        filter_taps.reshape(4, 1, W),
        conv_bias.reshape(1, W),
        recur_bias.reshape(1, W),
        entry_bias.reshape(1, W),
        forget_rate.reshape(1, W),
        output_weight,
    )


def solution(mesh):
    fine = Mesh(mesh.devices.reshape(4, 2, 4, 4), ("x", "c", "z", "y"))
    SP, TP = ("x", "c"), ("z", "y")
    both = SP + TP
    placed = (
        P(None, both, None),
        P(),
        P(None, TP),
        P(None, TP),
        P(None, TP),
        P(TP),
        P(TP, None, None),
        P(TP),
        P(TP, None, None),
        P(TP),
        P(TP),
        P(TP, None),
    )
    return jax.shard_map(
        per_device, mesh=fine, in_specs=placed, out_specs=P(None, both, None), check_vma=False
    )
```

```python
import jax
import jax.numpy as jnp
from jax import lax
from jax.experimental import pallas as pl
from jax.experimental.pallas import tpu as pltpu
from jax.sharding import Mesh
from jax.sharding import PartitionSpec as P

MESH = pl.DeviceIdType.MESH
EPS = 1e-06
POWER = 8.0
SEQS = 4
TOK = 16
STR = 64
D = 2048
W = 128
NB = 4
CH = NB * W
ROWS = SEQS * STR
AROWS = D + 2 * W
PIECE = ((AROWS // 16, 0), (AROWS // 16, AROWS // 2), (D // 8, 0), (W // 8, 0))
f32 = jnp.float32
bf16 = jnp.bfloat16


class Slots:
    def __init__(self):
        self.index = {}

    def __call__(self, *key):
        return self.index.setdefault(key, len(self.index))


N_COPIES = 74
N_SENDS = 16
N_LOCAL = 7
VMEM_LIMIT = 67043328


def neg_expm1(t):
    s = 1.0 + t * (1.0 / 8.0)
    for n in (7.0, 6.0, 5.0, 4.0, 3.0, 2.0):
        s = 1.0 + t * (1.0 / n) * s
    return jnp.where(t > -0.5, -t * s, 1.0 - jnp.exp(t))


def sigmoid(v):
    return 1.0 / (1.0 + jnp.exp(-v))


def kernel(
    tok_ref,
    gain_ref,
    w1_ref,
    w2_ref,
    rw_ref,
    ew_ref,
    taps_ref,
    cb_ref,
    rb_ref,
    eb_ref,
    rate_ref,
    wo_ref,
    out_ref,
    gain,
    tr,
    nt,
    wa,
    wv,
    wog,
    sm,
    ci,
    hs,
    hr,
    cv,
    lg,
    de,
    pu,
    sg,
    gt,
    g16,
    s_own,
    l1,
    t_own,
    l2,
    pb,
    pf,
    rd,
    rb,
    ob,
    ssem,
    rsem,
    lsem,
):
    X = lax.axis_index("x")
    C = lax.axis_index("c")
    Z = lax.axis_index("z")
    Y = lax.axis_index("y")
    g = X * 2 + C
    par = lax.rem(X, 2)

    def mod4(v):
        return lax.rem(v + 8, 4)

    def gdev(v):
        return {"x": v // 2, "c": lax.rem(v, 2)}

    nxt_z = mod4(Z + 1)
    nxt_g = lax.rem(g + jnp.where(Z == 3, 1, 0), 8)
    prv_z = mod4(Z - 1)
    prv_g = lax.rem(g + 8 - jnp.where(Z == 0, 1, 0), 8)
    nxt = {"x": nxt_g // 2, "c": lax.rem(nxt_g, 2), "z": nxt_z}
    prv = {"x": prv_g // 2, "c": lax.rem(prv_g, 2), "z": prv_z}
    yp, ym = {"y": mod4(Y + 1)}, {"y": mod4(Y - 1)}
    zp, zm = {"z": nxt_z}, {"z": prv_z}
    xp, xm = {"x": mod4(X + 1)}, {"x": mod4(X - 1)}
    mate = {"c": 1 - C}

    slot = Slots()
    local = Slots()
    scopes = []

    def mark(name):
        if scopes:
            scopes.pop().__exit__(None, None, None)
        if name:
            scopes.append(jax.named_scope(name))
            scopes[-1].__enter__()

    def remote(out, key, src, dst, dev):
        return pltpu.make_async_remote_copy(
            src_ref=src,
            dst_ref=dst,
            send_sem=ssem.at[out],
            recv_sem=rsem.at[slot(*key)],
            device_id=dev,
            device_id_type=MESH,
        )

    def send(out, key, src, dst, dev):
        remote(out, key, src, dst, dev).start()

    def arrived(key, dst):
        remote(0, key, dst, dst, mate).wait_recv()

    def left(out, ref):
        remote(out, ("t", 0, 0), ref, ref, mate).wait_send()

    def fetch(key, src, dst):
        copy = pltpu.make_async_copy(src, dst, lsem.at[local(key)])
        copy.start()
        return copy

    mark("own")
    own_tok = tr.at[:, pl.ds(pl.multiple_of(Y * TOK, TOK), TOK), :]
    c_tok = fetch("tok", tok_ref, own_tok)
    fetch("wa", w1_ref, wa.at[Z, pl.ds(0, D)])
    fetch("wa", rw_ref.at[0], wa.at[Z, pl.ds(D, W)])
    fetch("wa", ew_ref.at[0], wa.at[Z, pl.ds(D + W, W)])
    fetch("sm", taps_ref, sm.at[Z, pl.ds(0, 4)])
    for n, ref in enumerate((cb_ref, rb_ref, eb_ref, rate_ref)):
        fetch("sm", ref, sm.at[Z, 4 + n])
    c_gain = fetch("gain", gain_ref, gain)
    c_wv = fetch("w2", w2_ref, wv.at[Z])
    c_wo = fetch("wo", wo_ref, wog.at[Z])

    l2[...] = jnp.zeros_like(l2)

    mark("barrier")
    barrier = pltpu.get_barrier_semaphore()
    partners = [yp, ym] + [{"z": mod4(Z + d)} for d in (1, 2, 3)]
    partners += [gdev(lax.rem(g + d, 8)) for d in range(1, 8)] + [nxt, prv]
    for dev in partners:
        pl.semaphore_signal(barrier, inc=1, device_id=dev, device_id_type=MESH)
    pl.semaphore_wait(barrier, len(partners))

    mark("tokens")
    def tok(y, half):
        return tr.at[pl.ds(2 * half, 2), pl.ds(pl.multiple_of(y * TOK, TOK), TOK), :]

    y_m, y_p, y_d = mod4(Y - 1), mod4(Y + 1), mod4(Y + 2)
    c_tok.wait()
    send(0, ("t", 0, 0), tok(Y, 0), tok(Y, 0), yp)
    send(0, ("t", 1, 1), tok(Y, 1), tok(Y, 1), ym)
    send(0, ("t", 0, 1), tok(Y, 1), tok(Y, 1), yp)
    send(0, ("t", 1, 0), tok(Y, 0), tok(Y, 0), ym)

    def piece(m, z, q, core, h):
        rows, base = PIECE[m]
        k = q * 4 + core * 2 + h
        place = pl.ds(pl.multiple_of(base + k * rows, 16), rows)
        if m == 3:
            return wog.at[z, place]
        return (wa, wa, wv)[m].at[z, place]

    blocks = (mod4(Z - 1), mod4(Z + 1), mod4(Z + 2))

    def own_send(m):
        for j, h, dev in ((0, 0, zp), (1, 1, zm), (0, 1, zp), (1, 0, zm)):
            ref = piece(m, Z, par, C, h)
            send(1 + m, ("z", m, j, h), ref, ref, dev)

    def z_event(m, j, h):
        ref = piece(m, blocks[j], par, C, h)
        arrived(("z", m, j, h), ref)
        if (j, h) == (0, 0):
            send(1 + m, ("z", m, 2, 0), ref, ref, zp)
        if (j, h) == (1, 1):
            send(1 + m, ("z", m, 2, 1), ref, ref, zm)
        send(1 + m, ("x", m, j, h), ref, ref, xp if h == 0 else xm)
        send(1 + m, ("d", m), ref, ref, mate)

    def x_event(m, j, h):
        ref = piece(m, blocks[j], 1 - par, C, h)
        arrived(("x", m, j, h), ref)
        send(1 + m, ("d", m), ref, ref, mate)

    def near_z(m):
        z_event(m, 0, 0)
        z_event(m, 1, 1)

    def next_z(m):
        z_event(m, 0, 1)
        z_event(m, 1, 0)

    def far_z(m):
        z_event(m, 2, 0)
        z_event(m, 2, 1)

    def near_x(m):
        x_event(m, 0, 0)
        x_event(m, 1, 1)

    def next_x(m):
        x_event(m, 0, 1)
        x_event(m, 1, 0)

    def far_x(m):
        x_event(m, 2, 0)
        x_event(m, 2, 1)

    def volume(m, parts):
        return (wa, wa, wv, wog)[m].at[pl.ds(0, parts // 6), pl.ds(0, PIECE[m][0] * 6)]

    mark("weights")
    pltpu.make_async_copy(wa.at[0], wa.at[0], lsem.at[local("wa")]).wait()
    own_send(0)
    own_send(1)
    pltpu.make_async_copy(sm.at[0], sm.at[0], lsem.at[local("sm")]).wait()
    for d in (1, 2, 3):
        send(5, ("s",), sm.at[Z], sm.at[Z], {"z": mod4(Z + d)})

    def norm(y, half):
        rows = pl.ds(pl.multiple_of(y * TOK, TOK), TOK)
        v = tr[pl.ds(2 * half, 2), rows, :].astype(f32)
        v = v * lax.rsqrt(jnp.mean(v * v, axis=-1, keepdims=True) + EPS)
        v = (v * gain[...].reshape(1, 1, D)).astype(bf16)
        for s in range(2):
            nt[pl.ds(pl.multiple_of((2 * half + s) * STR + y * TOK, TOK), TOK), :] = v[s]

    mark("norm0")
    c_gain.wait()
    norm(Y, 0)
    norm(Y, 1)
    mark("net0")
    near_z(0)
    near_z(1)
    c_wv.wait()
    own_send(2)
    mark("net1")
    arrived(("t", 0, 0), tok(y_m, 0))
    send(0, ("t", 2, 0), tok(y_m, 0), tok(y_m, 0), yp)
    arrived(("t", 1, 1), tok(y_p, 1))
    send(0, ("t", 2, 1), tok(y_p, 1), tok(y_p, 1), ym)
    mark("net2")
    next_z(0)
    next_z(1)
    mark("norm1")
    norm(y_m, 0)
    norm(y_p, 1)
    mark("net3")
    near_x(0)
    near_x(1)
    far_z(0)
    far_z(1)
    next_x(0)
    next_x(1)
    mark("net3t")
    arrived(("t", 0, 1), tok(y_m, 1))
    arrived(("t", 1, 0), tok(y_p, 0))
    mark("norm2")
    norm(y_m, 1)
    norm(y_p, 0)
    mark("net4")
    near_z(2)
    c_wo.wait()
    own_send(3)
    mark("net5")
    far_x(0)
    far_x(1)
    mark("net5t")
    arrived(("t", 2, 0), tok(y_d, 0))
    norm(y_d, 0)
    arrived(("t", 2, 1), tok(y_d, 1))
    norm(y_d, 1)
    mark("d0")
    arrived(("d", 0), volume(0, 12))
    arrived(("d", 1), volume(1, 12))

    mark("matmul1")

    def pair(ref, b):
        rhs = jnp.concatenate([ref[b, 0:D, :], ref[b + 1, 0:D, :]], axis=1)
        return jnp.dot(nt[...], rhs, preferred_element_type=f32).astype(bf16).astype(f32)

    for b in range(0, NB, 2):
        part = pair(wa, b)
        ci[b] = part[:, 0:W]
        ci[b + 1] = part[:, W : 2 * W]
        for n in (b, b + 1):
            for s in range(SEQS):
                last = part[s * STR + STR - 8 : s * STR + STR, (n - b) * W : (n - b + 1) * W]
                hs[n, s * 8 : s * 8 + 8, :] = last
    send(6, ("h",), hs, hr, nxt)
    mark("net6")
    next_z(2)
    arrived(("s",), sm.at[pl.ds(0, 3)])

    mark("conv")
    lane_row = lax.broadcasted_iota(jnp.int32, (8, W), 0)

    def convolve(b, at):
        acc = jnp.broadcast_to(sm[b, 4], (8, W))
        for k in range(4):
            acc = acc + at(k - 3) * sm[b, k]
        return acc

    for b in range(NB):
        for s in range(SEQS):
            x = [ci[b, pl.ds(s * STR + i, 8, stride=8), :] for i in range(8)]
            prev = {i - 8: pltpu.roll(x[i], 1, 0) for i in (5, 6, 7)}
            rows = []
            for i in range(8):
                rows.append(convolve(b, lambda n: x[i + n] if i + n >= 0 else prev[i + n]))
            cv[pl.ds(s * STR, STR), b * W : (b + 1) * W] = jnp.concatenate(rows, axis=0).astype(bf16)

    mark("gates")

    def gates(b, logit_r, logit_e, conv):
        r_gate = sigmoid(logit_r + sm[b, 5])
        e_gate = sigmoid(logit_e + sm[b, 6])
        log_decay = (-POWER * r_gate) * sm[b, 7]
        push = jnp.sqrt(neg_expm1(2.0 * log_decay)) * (e_gate * conv.astype(f32))
        return jnp.exp(log_decay), push

    def gate_dots(b, conv):
        return [
            jnp.dot(conv, wa[b, D + n * W : D + (n + 1) * W, :], preferred_element_type=f32)
            for n in range(2)
        ]

    for b in range(NB):
        cols = slice(b * W, (b + 1) * W)
        lg[0], lg[1] = gate_dots(b, cv[:, cols])
        for s in range(SEQS):
            rows = slice(s * STR, (s + 1) * STR)
            de[b, rows, :], pu[b, rows, :] = gates(b, lg[0, rows, :], lg[1, rows, :], cv[rows, cols])

    mark("net7")
    far_z(2)
    near_x(2)
    near_z(3)
    mark("halo")
    arrived(("h",), hr)
    mark("redo")
    start = jnp.logical_and(g == 0, Z == 0)
    for b in range(NB):
        tiles = []
        for s in range(SEQS):
            behind = jnp.where(start, 0.0, hr[b, s * 8 : s * 8 + 8, :])
            here = ci[b, s * STR : s * STR + 8, :]

            def at(n):
                if n == 0:
                    return here
                return jnp.where(lane_row < -n, pltpu.roll(behind, -n, 0), pltpu.roll(here, -n, 0))

            tiles.append(convolve(b, at))
        conv = jnp.concatenate(tiles, axis=0).astype(bf16)
        decay, push = gates(b, *gate_dots(b, conv), conv)
        for s in range(SEQS):
            chain = pl.ds(s * STR, 8, stride=8)
            de[b, chain, :] = decay[s * 8 : s * 8 + 8]
            pu[b, chain, :] = push[s * 8 : s * 8 + 8]

    mark("scan")
    ends = [[None] * SEQS for _ in range(NB)]
    for b in range(NB):
        cols = slice(b * W, (b + 1) * W)
        tot_a, tot_h = [], []
        for s in range(SEQS):
            a = de[b, s * STR : s * STR + 8, :]
            h = pu[b, s * STR : s * STR + 8, :]
            for i in range(1, 8):
                at = slice(s * STR + i * 8, s * STR + i * 8 + 8)
                step = de[b, at, :]
                h = step * h + pu[b, at, :]
                a = step * a
                de[b, at, :] = a
                pu[b, at, :] = h
            for n in (1, 2, 4):
                keep = lane_row >= n
                a_in = jnp.where(keep, pltpu.roll(a, n, 0), 1.0)
                h_in = jnp.where(keep, pltpu.roll(h, n, 0), 0.0)
                h = a * h_in + h
                a = a * a_in
            tot_a.append(a[7:8])
            tot_h.append(h[7:8])
            ends[b][s] = (
                jnp.where(lane_row >= 1, pltpu.roll(a, 1, 0), 1.0),
                jnp.where(lane_row >= 1, pltpu.roll(h, 1, 0), 0.0),
            )
        s_own[:, cols] = jnp.concatenate(tot_a + tot_h, axis=0).astype(bf16)

    mark("states")
    for d in (1, 2, 3):
        send(7, ("e",), s_own, l1.at[Z], {"z": mod4(Z + d)})
    l1[Z] = s_own[...]
    next_x(2)
    far_x(2)
    next_z(3)
    mark("states1")
    arrived(("e",), l1.at[pl.ds(0, 3)])
    total_a, total_h = l1[0, 0:4].astype(f32), l1[0, 4:8].astype(f32)
    for k in range(1, 4):
        ka, kh = l1[k, 0:4].astype(f32), l1[k, 4:8].astype(f32)
        total_h = ka * total_h + kh
        total_a = ka * total_a
    t_own[...] = jnp.concatenate([total_a, total_h], axis=0).astype(bf16)

    def to_group(d):
        return remote(8 + d, ("g", d), t_own, l2.at[g], gdev(lax.rem(g + d, 8)))

    for d in range(1, 8):

        @pl.when(g + d < 8)
        def _():
            to_group(d).start()

    mark("net8")
    far_z(3)
    near_x(3)
    next_x(3)
    arrived(("d", 2), volume(2, 12))
    mark("valve")
    for b in range(0, NB, 2):
        v = pair(wv, b)
        v = v / (1.0 + jnp.exp(-v))
        sg[b] = v[:, 0:W]
        sg[b + 1] = v[:, W : 2 * W]
    far_x(3)
    mark("states2")
    for d in range(1, 8):

        @pl.when(g - d >= 0)
        def _():
            arrived(("g", d), l2.at[lax.rem(g - d + 8, 8)])

    mark("entering")
    state = jnp.zeros((SEQS, CH), f32)
    for k in range(7):
        state = jnp.where(k < g, l2[k, 0:4].astype(f32) * state + l2[k, 4:8].astype(f32), state)
    for k in range(3):
        state = jnp.where(k < Z, l1[k, 0:4].astype(f32) * state + l1[k, 4:8].astype(f32), state)

    mark("gated")
    for b in range(NB):
        cols = slice(b * W, (b + 1) * W)
        for s in range(SEQS):
            chain_a, chain_h = ends[b][s]
            enter = chain_a * jnp.broadcast_to(state[s : s + 1, cols], (8, W)) + chain_h
            for i in range(8):
                at = s * STR + i * 8
                h = de[b, at : at + 8, :] * enter + pu[b, at : at + 8, :]
                places = pl.ds(s * STR + i, 8, stride=8)
                gt[b, places, :] = h * sg[b, places, :]
        g16[:, cols] = gt[b].astype(bf16)

    mark("d2")
    arrived(("d", 3), volume(3, 12))

    def product(y):
        lhs = jnp.concatenate(
            [g16[pl.ds(pl.multiple_of(s * STR + y * TOK, TOK), TOK), :] for s in range(SEQS)], axis=0
        )
        return jnp.dot(lhs, wog[...].reshape(CH, D), preferred_element_type=f32)

    mark("prod0")
    p = product(y_d).astype(bf16).reshape(SEQS, TOK, D)
    pb[0] = p
    send(8, ("r", 0), pb.at[0, pl.ds(0, 2)], rd.at[0], ym)
    send(8, ("r", 1), pb.at[0, pl.ds(2, 2)], rd.at[1], yp)
    mark("prod1")
    p = product(y_p).reshape(SEQS, TOK, D)
    pb[1, 0:2] = p[0:2].astype(bf16)
    send(8, ("r", 2), pb.at[1, pl.ds(0, 2)], rb.at[0, pl.ds(0, 2)], yp)
    pf[1] = p[2:4]
    p = product(y_m).reshape(SEQS, TOK, D)
    pb[2, 2:4] = p[2:4].astype(bf16)
    send(8, ("r", 3), pb.at[2, pl.ds(2, 2)], rb.at[1, pl.ds(2, 2)], ym)
    pf[0] = p[0:2]
    mine = product(Y).reshape(SEQS, TOK, D)
    mark("red1")
    arrived(("r", 1), rd.at[1])
    pb[1, 2:4] = (pf[1] + rd[1].astype(f32)).astype(bf16)
    send(8, ("r", 4), pb.at[1, pl.ds(2, 2)], rb.at[0, pl.ds(2, 2)], yp)
    arrived(("r", 0), rd.at[0])
    pb[2, 0:2] = (pf[0] + rd[0].astype(f32)).astype(bf16)
    send(8, ("r", 5), pb.at[2, pl.ds(0, 2)], rb.at[1, pl.ds(0, 2)], ym)
    mark("red2")
    arrived(("r", 2), rb.at[0, pl.ds(0, 2)])
    arrived(("r", 3), rb.at[1, pl.ds(2, 2)])
    arrived(("r", 4), rb.at[0, pl.ds(2, 2)])
    arrived(("r", 5), rb.at[1, pl.ds(0, 2)])
    mark("final")
    ob[...] = (mine + rb[0].astype(f32) + rb[1].astype(f32)).astype(bf16)
    c_out = fetch("out", ob, out_ref)

    mark("drain")
    left(0, tr.at[pl.ds(0, 3)])
    for m in range(4):
        left(1 + m, volume(m, 24))
    left(5, sm.at[pl.ds(0, 3)])
    left(6, hs)
    left(7, l1.at[pl.ds(0, 3)])
    left(8, pb)
    for d in range(1, 8):

        @pl.when(g + d < 8)
        def _():
            to_group(d).wait_send()

    mark("outwait")
    c_out.wait()
    assert len(slot.index) <= N_COPIES and len(local.index) <= N_LOCAL
    mark(None)


def per_device(
    tokens,
    norm_gain,
    entry_projection,
    valve_projection,
    filter_taps,
    conv_bias,
    recur_weight,
    recur_bias,
    entry_weight,
    entry_bias,
    forget_rate,
    output_weight,
):
    hbm = pl.BlockSpec(memory_space=pltpu.HBM)
    return pl.pallas_call(
        kernel,
        name="layer",
        out_shape=jax.ShapeDtypeStruct((SEQS, TOK, D), bf16),
        in_specs=[hbm] * 12,
        out_specs=hbm,
        scratch_shapes=[
            pltpu.VMEM((1, D), f32),
            pltpu.VMEM((SEQS, STR, D), bf16),
            pltpu.VMEM((ROWS, D), bf16),
            pltpu.VMEM((NB, AROWS, W), bf16),
            pltpu.VMEM((NB, D, W), bf16),
            pltpu.VMEM((NB, W, D), bf16),
            pltpu.VMEM((NB, 8, 1, W), f32),
            pltpu.VMEM((NB, ROWS, W), f32),
            pltpu.VMEM((NB, 32, W), f32),
            pltpu.VMEM((NB, 32, W), f32),
            pltpu.VMEM((ROWS, CH), bf16),
            pltpu.VMEM((2, ROWS, W), f32),
            pltpu.VMEM((NB, ROWS, W), f32),
            pltpu.VMEM((NB, ROWS, W), f32),
            pltpu.VMEM((NB, ROWS, W), f32),
            pltpu.VMEM((NB, ROWS, W), f32),
            pltpu.VMEM((ROWS, CH), bf16),
            pltpu.VMEM((8, CH), bf16),
            pltpu.VMEM((4, 8, CH), bf16),
            pltpu.VMEM((8, CH), bf16),
            pltpu.VMEM((8, 8, CH), bf16),
            pltpu.VMEM((3, SEQS, TOK, D), bf16),
            pltpu.VMEM((2, 2, TOK, D), f32),
            pltpu.VMEM((2, 2, TOK, D), bf16),
            pltpu.VMEM((2, SEQS, TOK, D), bf16),
            pltpu.VMEM((SEQS, TOK, D), bf16),
            pltpu.SemaphoreType.DMA((N_SENDS,)),
            pltpu.SemaphoreType.DMA((N_COPIES,)),
            pltpu.SemaphoreType.DMA((N_LOCAL,)),
        ],
        compiler_params=pltpu.CompilerParams(
            collective_id=0, has_side_effects=True, vmem_limit_bytes=VMEM_LIMIT
        ),
    )(
        tokens,
        norm_gain.reshape(1, D),
        entry_projection,
        valve_projection,
        recur_weight,
        entry_weight,
        filter_taps.reshape(4, 1, W),
        conv_bias.reshape(1, W),
        recur_bias.reshape(1, W),
        entry_bias.reshape(1, W),
        forget_rate.reshape(1, W),
        output_weight,
    )


def solution(mesh):
    fine = Mesh(mesh.devices.reshape(4, 2, 4, 4), ("x", "c", "z", "y"))
    SP, TP = ("x", "c"), ("z", "y")
    both = SP + TP
    placed = (
        P(None, both, None),
        P(),
        P(None, TP),
        P(None, TP),
        P(None, TP),
        P(TP),
        P(TP, None, None),
        P(TP),
        P(TP, None, None),
        P(TP),
        P(TP),
        P(TP, None),
    )
    return jax.shard_map(
        per_device, mesh=fine, in_specs=placed, out_specs=P(None, both, None), check_vma=False
    )
```

```python
import jax
import jax.numpy as jnp
from jax import lax
from jax.experimental import pallas as pl
from jax.experimental.pallas import tpu as pltpu
from jax.sharding import Mesh
from jax.sharding import PartitionSpec as P

MESH = pl.DeviceIdType.MESH
EPS = 1e-06
POWER = 8.0
TINY = 1e-37
SEQS = 4
TOK = 16
STR = 64
D = 2048
W = 128
NB = 4
CH = NB * W
ROWS = SEQS * STR
AROWS = D + 2 * W
PIECE = ((AROWS // 16, 0), (AROWS // 16, AROWS // 2), (D // 8, 0), (W // 8, 0))
f32 = jnp.float32
bf16 = jnp.bfloat16


class Slots:
    def __init__(self):
        self.index = {}

    def __call__(self, *key):
        return self.index.setdefault(key, len(self.index))


N_COPIES = 74
N_SENDS = 16
N_LOCAL = 7
VMEM_LIMIT = 66700000


def neg_expm1(t):
    s = 1.0 + t * (1.0 / 8.0)
    for n in (7.0, 6.0, 5.0, 4.0, 3.0, 2.0):
        s = 1.0 + t * (1.0 / n) * s
    return jnp.where(t > -0.5, -t * s, 1.0 - jnp.exp(t))


def sigmoid(v):
    return 1.0 / (1.0 + jnp.exp(-v))


def kernel(
    tok_ref,
    gain_ref,
    w1_ref,
    w2_ref,
    rw_ref,
    ew_ref,
    taps_ref,
    cb_ref,
    rb_ref,
    eb_ref,
    rate_ref,
    wo_ref,
    out_ref,
    gain,
    tr,
    nt,
    wa,
    wv,
    wog,
    sm,
    ci,
    hs,
    hr,
    cv,
    lg,
    de,
    pu,
    sg,
    gt,
    g16,
    s_own,
    l1,
    t_own,
    l2,
    pb,
    pf,
    rd,
    rb,
    ssem,
    rsem,
    lsem,
):
    X = lax.axis_index("x")
    C = lax.axis_index("c")
    Z = lax.axis_index("z")
    Y = lax.axis_index("y")
    g = X * 2 + C
    par = lax.rem(X, 2)

    def mod4(v):
        return lax.rem(v + 8, 4)

    def gdev(v):
        return {"x": v // 2, "c": lax.rem(v, 2)}

    nxt_z = mod4(Z + 1)
    nxt_g = lax.rem(g + jnp.where(Z == 3, 1, 0), 8)
    prv_z = mod4(Z - 1)
    prv_g = lax.rem(g + 8 - jnp.where(Z == 0, 1, 0), 8)
    nxt = {"x": nxt_g // 2, "c": lax.rem(nxt_g, 2), "z": nxt_z}
    prv = {"x": prv_g // 2, "c": lax.rem(prv_g, 2), "z": prv_z}
    yp, ym = {"y": mod4(Y + 1)}, {"y": mod4(Y - 1)}
    zp, zm = {"z": nxt_z}, {"z": prv_z}
    xp, xm = {"x": mod4(X + 1)}, {"x": mod4(X - 1)}
    mate = {"c": 1 - C}

    slot = Slots()
    local = Slots()
    scopes = []

    def mark(name):
        if scopes:
            scopes.pop().__exit__(None, None, None)
        if name:
            scopes.append(jax.named_scope(name))
            scopes[-1].__enter__()

    def remote(out, key, src, dst, dev):
        return pltpu.make_async_remote_copy(
            src_ref=src,
            dst_ref=dst,
            send_sem=ssem.at[out],
            recv_sem=rsem.at[slot(*key)],
            device_id=dev,
            device_id_type=MESH,
        )

    def send(out, key, src, dst, dev):
        remote(out, key, src, dst, dev).start()

    def arrived(key, dst):
        remote(0, key, dst, dst, mate).wait_recv()

    def left(out, ref):
        remote(out, ("t", 0, 0), ref, ref, mate).wait_send()

    def fetch(key, src, dst):
        copy = pltpu.make_async_copy(src, dst, lsem.at[local(key)])
        copy.start()
        return copy

    mark("own")
    own_tok = tr.at[:, pl.ds(pl.multiple_of(Y * TOK, TOK), TOK), :]
    c_tok = fetch("tok", tok_ref, own_tok)
    fetch("wa", w1_ref, wa.at[Z, pl.ds(0, D)])
    fetch("wa", rw_ref.at[0], wa.at[Z, pl.ds(D, W)])
    fetch("wa", ew_ref.at[0], wa.at[Z, pl.ds(D + W, W)])
    fetch("sm", taps_ref, sm.at[Z, pl.ds(0, 4)])
    for n, ref in enumerate((cb_ref, rb_ref, eb_ref, rate_ref)):
        fetch("sm", ref, sm.at[Z, 4 + n])
    c_gain = fetch("gain", gain_ref, gain)
    c_wv = fetch("w2", w2_ref, wv.at[Z])
    c_wo = fetch("wo", wo_ref, wog.at[Z])

    l2[...] = jnp.zeros_like(l2)

    mark("barrier")
    barrier = pltpu.get_barrier_semaphore()
    partners = [yp, ym] + [{"z": mod4(Z + d)} for d in (1, 2, 3)]
    partners += [gdev(lax.rem(g + d, 8)) for d in range(1, 8)] + [nxt, prv]
    for dev in partners:
        pl.semaphore_signal(barrier, inc=1, device_id=dev, device_id_type=MESH)
    pl.semaphore_wait(barrier, len(partners))

    mark("tokens")
    def tok(y, half):
        return tr.at[pl.ds(2 * half, 2), pl.ds(pl.multiple_of(y * TOK, TOK), TOK), :]

    y_m, y_p, y_d = mod4(Y - 1), mod4(Y + 1), mod4(Y + 2)
    c_tok.wait()
    send(0, ("t", 0, 0), tok(Y, 0), tok(Y, 0), yp)
    send(0, ("t", 1, 1), tok(Y, 1), tok(Y, 1), ym)
    send(0, ("t", 0, 1), tok(Y, 1), tok(Y, 1), yp)
    send(0, ("t", 1, 0), tok(Y, 0), tok(Y, 0), ym)

    def piece(m, z, q, core, h):
        rows, base = PIECE[m]
        k = q * 4 + core * 2 + h
        place = pl.ds(pl.multiple_of(base + k * rows, 16), rows)
        if m == 3:
            return wog.at[z, place]
        return (wa, wa, wv)[m].at[z, place]

    blocks = (mod4(Z - 1), mod4(Z + 1), mod4(Z + 2))

    def own_send(m):
        for j, h, dev in ((0, 0, zp), (1, 1, zm), (0, 1, zp), (1, 0, zm)):
            ref = piece(m, Z, par, C, h)
            send(1 + m, ("z", m, j, h), ref, ref, dev)

    def z_event(m, j, h):
        ref = piece(m, blocks[j], par, C, h)
        arrived(("z", m, j, h), ref)
        if (j, h) == (0, 0):
            send(1 + m, ("z", m, 2, 0), ref, ref, zp)
        if (j, h) == (1, 1):
            send(1 + m, ("z", m, 2, 1), ref, ref, zm)
        send(1 + m, ("x", m, j, h), ref, ref, xp if h == 0 else xm)
        send(1 + m, ("d", m), ref, ref, mate)

    def x_event(m, j, h):
        ref = piece(m, blocks[j], 1 - par, C, h)
        arrived(("x", m, j, h), ref)
        send(1 + m, ("d", m), ref, ref, mate)

    def near_z(m):
        z_event(m, 0, 0)
        z_event(m, 1, 1)

    def next_z(m):
        z_event(m, 0, 1)
        z_event(m, 1, 0)

    def far_z(m):
        z_event(m, 2, 0)
        z_event(m, 2, 1)

    def near_x(m):
        x_event(m, 0, 0)
        x_event(m, 1, 1)

    def next_x(m):
        x_event(m, 0, 1)
        x_event(m, 1, 0)

    def far_x(m):
        x_event(m, 2, 0)
        x_event(m, 2, 1)

    def volume(m, parts):
        return (wa, wa, wv, wog)[m].at[pl.ds(0, parts // 6), pl.ds(0, PIECE[m][0] * 6)]

    mark("weights")
    pltpu.make_async_copy(wa.at[0], wa.at[0], lsem.at[local("wa")]).wait()
    own_send(0)
    own_send(1)
    pltpu.make_async_copy(sm.at[0], sm.at[0], lsem.at[local("sm")]).wait()
    for d in (1, 2, 3):
        send(5, ("s",), sm.at[Z], sm.at[Z], {"z": mod4(Z + d)})

    def norm(y, half):
        rows = pl.ds(pl.multiple_of(y * TOK, TOK), TOK)
        v = tr[pl.ds(2 * half, 2), rows, :].astype(f32)
        v = v * lax.rsqrt(jnp.mean(v * v, axis=-1, keepdims=True) + EPS)
        v = (v * gain[...].reshape(1, 1, D)).astype(bf16)
        for s in range(2):
            nt[pl.ds(pl.multiple_of((2 * half + s) * STR + y * TOK, TOK), TOK), :] = v[s]

    mark("norm0")
    c_gain.wait()
    norm(Y, 0)
    norm(Y, 1)
    mark("net0")
    near_z(0)
    near_z(1)
    c_wv.wait()
    own_send(2)
    c_wo.wait()
    own_send(3)
    mark("net1")
    arrived(("t", 0, 0), tok(y_m, 0))
    send(0, ("t", 2, 0), tok(y_m, 0), tok(y_m, 0), yp)
    arrived(("t", 1, 1), tok(y_p, 1))
    send(0, ("t", 2, 1), tok(y_p, 1), tok(y_p, 1), ym)
    mark("net2")
    next_z(0)
    next_z(1)
    mark("norm1")
    norm(y_m, 0)
    norm(y_p, 1)
    mark("net3")
    near_x(0)
    near_x(1)
    far_z(0)
    far_z(1)
    next_x(0)
    next_x(1)
    mark("net3t")
    arrived(("t", 0, 1), tok(y_m, 1))
    arrived(("t", 1, 0), tok(y_p, 0))
    mark("norm2")
    norm(y_m, 1)
    norm(y_p, 0)
    mark("net4")
    near_z(2)
    mark("net5")
    far_x(0)
    far_x(1)
    mark("net5t")
    arrived(("t", 2, 0), tok(y_d, 0))
    norm(y_d, 0)
    arrived(("t", 2, 1), tok(y_d, 1))
    norm(y_d, 1)
    mark("d0")
    arrived(("d", 0), volume(0, 12))
    arrived(("d", 1), volume(1, 12))

    mark("matmul1")

    def pair(ref, b):
        rhs = jnp.concatenate([ref[b, 0:D, :], ref[b + 1, 0:D, :]], axis=1)
        return jnp.dot(nt[...], rhs, preferred_element_type=f32).astype(bf16).astype(f32)

    for b in range(0, NB, 2):
        part = pair(wa, b)
        ci[b] = part[:, 0:W]
        ci[b + 1] = part[:, W : 2 * W]
        for n in (b, b + 1):
            for s in range(SEQS):
                last = part[s * STR + STR - 8 : s * STR + STR, (n - b) * W : (n - b + 1) * W]
                hs[n, s * 8 : s * 8 + 8, :] = last.astype(bf16)
    send(6, ("h",), hs, hr, nxt)
    mark("net6")
    next_z(2)
    near_z(3)
    near_x(2)
    arrived(("s",), sm.at[pl.ds(0, 3)])

    mark("conv")
    lane_row = lax.broadcasted_iota(jnp.int32, (8, W), 0)

    def convolve(b, at):
        acc = jnp.broadcast_to(sm[b, 4], (8, W))
        for k in range(4):
            acc = acc + at(k - 3) * sm[b, k]
        return acc

    for b in range(NB):
        for s in range(SEQS):
            x = [ci[b, pl.ds(s * STR + i, 8, stride=8), :] for i in range(8)]
            prev = {i - 8: pltpu.roll(x[i], 1, 0) for i in (5, 6, 7)}
            rows = []
            for i in range(8):
                rows.append(convolve(b, lambda n: x[i + n] if i + n >= 0 else prev[i + n]))
            cv[pl.ds(s * STR, STR), b * W : (b + 1) * W] = jnp.concatenate(rows, axis=0).astype(bf16)

    mark("gates")

    def gates(b, logit_r, logit_e, conv):
        r_gate = sigmoid(logit_r + sm[b, 5])
        e_gate = sigmoid(logit_e + sm[b, 6])
        log_decay = (-POWER * r_gate) * sm[b, 7]
        push = jnp.sqrt(neg_expm1(2.0 * log_decay)) * (e_gate * conv.astype(f32))
        return jnp.exp(log_decay), push

    def gate_dots(b, conv):
        return [
            jnp.dot(conv, wa[b, D + n * W : D + (n + 1) * W, :], preferred_element_type=f32)
            for n in range(2)
        ]

    for b in range(NB):
        cols = slice(b * W, (b + 1) * W)
        lg[0], lg[1] = gate_dots(b, cv[:, cols])
        for s in range(SEQS):
            rows = slice(s * STR, (s + 1) * STR)
            de[b, rows, :], pu[b, rows, :] = gates(b, lg[0, rows, :], lg[1, rows, :], cv[rows, cols])

    mark("net7")
    next_z(3)
    next_x(2)
    far_z(2)
    near_x(3)
    mark("halo")
    arrived(("h",), hr)
    mark("redo")
    start = jnp.logical_and(g == 0, Z == 0)
    for b in range(NB):
        tiles = []
        for s in range(SEQS):
            behind = jnp.where(start, 0.0, hr[b, s * 8 : s * 8 + 8, :].astype(f32))
            here = ci[b, s * STR : s * STR + 8, :]

            def at(n):
                if n == 0:
                    return here
                return jnp.where(lane_row < -n, pltpu.roll(behind, -n, 0), pltpu.roll(here, -n, 0))

            tiles.append(convolve(b, at))
        conv = jnp.concatenate(tiles, axis=0).astype(bf16)
        decay, push = gates(b, *gate_dots(b, conv), conv)
        for s in range(SEQS):
            chain = pl.ds(s * STR, 8, stride=8)
            de[b, chain, :] = decay[s * 8 : s * 8 + 8]
            pu[b, chain, :] = push[s * 8 : s * 8 + 8]

    mark("scan")
    ends = [[None] * SEQS for _ in range(NB)]
    for b in range(NB):
        cols = slice(b * W, (b + 1) * W)
        tot_a, tot_h = [], []
        for s in range(SEQS):
            a = de[b, s * STR : s * STR + 8, :]
            h = pu[b, s * STR : s * STR + 8, :]
            for i in range(1, 8):
                at = slice(s * STR + i * 8, s * STR + i * 8 + 8)
                step = de[b, at, :]
                h = step * h + pu[b, at, :]
                a = step * a
                de[b, at, :] = a
                pu[b, at, :] = h
            for n in (1, 2, 4):
                keep = lane_row >= n
                a_in = jnp.where(keep, pltpu.roll(a, n, 0), 1.0)
                h_in = jnp.where(keep, pltpu.roll(h, n, 0), 0.0)
                h = a * h_in + h
                a = a * a_in
            tot_a.append(a[7:8])
            tot_h.append(h[7:8])
            ends[b][s] = (
                jnp.where(lane_row >= 1, pltpu.roll(a, 1, 0), 1.0),
                jnp.where(lane_row >= 1, pltpu.roll(h, 1, 0), 0.0),
            )
        tot_a = [jnp.log(jnp.maximum(a, TINY)) for a in tot_a]
        s_own[:, cols] = jnp.concatenate(tot_a + tot_h, axis=0).astype(bf16)

    mark("states")
    for d in (1, 2, 3):
        send(7, ("e",), s_own, l1.at[Z], {"z": mod4(Z + d)})
    l1[Z] = s_own[...]
    far_z(3)
    next_x(3)
    far_x(2)
    mark("states1")
    arrived(("e",), l1.at[pl.ds(0, 3)])
    total_a, total_h = l1[0, 0:4].astype(f32), l1[0, 4:8].astype(f32)
    for k in range(1, 4):
        ka, kh = l1[k, 0:4].astype(f32), l1[k, 4:8].astype(f32)
        total_h = jnp.exp(ka) * total_h + kh
        total_a = ka + total_a
    t_own[...] = jnp.concatenate([total_a, total_h], axis=0).astype(bf16)

    def to_group(d):
        return remote(8 + d, ("g", d), t_own, l2.at[g], gdev(lax.rem(g + d, 8)))

    for d in range(1, 8):

        @pl.when(g + d < 8)
        def _():
            to_group(d).start()

    mark("net8")
    far_x(3)
    arrived(("d", 2), volume(2, 12))
    mark("valve")
    for b in range(0, NB, 2):
        v = pair(wv, b)
        v = v / (1.0 + jnp.exp(-v))
        sg[b] = v[:, 0:W]
        sg[b + 1] = v[:, W : 2 * W]
    mark("states2")
    for d in range(1, 8):

        @pl.when(g - d >= 0)
        def _():
            arrived(("g", d), l2.at[lax.rem(g - d + 8, 8)])

    mark("entering")
    state = jnp.zeros((SEQS, CH), f32)
    for k in range(7):
        state = jnp.where(k < g, jnp.exp(l2[k, 0:4].astype(f32)) * state + l2[k, 4:8].astype(f32), state)
    for k in range(3):
        state = jnp.where(k < Z, jnp.exp(l1[k, 0:4].astype(f32)) * state + l1[k, 4:8].astype(f32), state)

    mark("gated")
    for b in range(NB):
        cols = slice(b * W, (b + 1) * W)
        for s in range(SEQS):
            chain_a, chain_h = ends[b][s]
            enter = chain_a * jnp.broadcast_to(state[s : s + 1, cols], (8, W)) + chain_h
            for i in range(8):
                at = s * STR + i * 8
                h = de[b, at : at + 8, :] * enter + pu[b, at : at + 8, :]
                places = pl.ds(s * STR + i, 8, stride=8)
                gt[b, places, :] = h * sg[b, places, :]
        g16[:, cols] = gt[b].astype(bf16)

    mark("d2")
    arrived(("d", 3), volume(3, 12))

    def product(y):
        lhs = jnp.concatenate(
            [g16[pl.ds(pl.multiple_of(s * STR + y * TOK, TOK), TOK), :] for s in range(SEQS)], axis=0
        )
        return jnp.dot(lhs, wog[...].reshape(CH, D), preferred_element_type=f32)

    mark("prod0")
    p = product(y_d).astype(bf16).reshape(SEQS, TOK, D)
    pb[0] = p
    send(8, ("r", 0), pb.at[0, pl.ds(0, 2)], rd.at[0], ym)
    send(8, ("r", 1), pb.at[0, pl.ds(2, 2)], rd.at[1], yp)
    mark("prod1")
    p = product(y_p).reshape(SEQS, TOK, D)
    pb[1, 0:2] = p[0:2].astype(bf16)
    send(8, ("r", 2), pb.at[1, pl.ds(0, 2)], rb.at[0, pl.ds(0, 2)], yp)
    pf[1] = p[2:4]
    p = product(y_m).reshape(SEQS, TOK, D)
    pb[2, 2:4] = p[2:4].astype(bf16)
    send(8, ("r", 3), pb.at[2, pl.ds(2, 2)], rb.at[1, pl.ds(2, 2)], ym)
    pf[0] = p[0:2]
    mine = product(Y).reshape(SEQS, TOK, D)
    mark("red1")
    arrived(("r", 1), rd.at[1])
    pb[1, 2:4] = (pf[1] + rd[1].astype(f32)).astype(bf16)
    send(8, ("r", 4), pb.at[1, pl.ds(2, 2)], rb.at[0, pl.ds(2, 2)], yp)
    arrived(("r", 0), rd.at[0])
    pb[2, 0:2] = (pf[0] + rd[0].astype(f32)).astype(bf16)
    send(8, ("r", 5), pb.at[2, pl.ds(0, 2)], rb.at[1, pl.ds(0, 2)], ym)
    mark("red2")
    arrived(("r", 2), rb.at[0, pl.ds(0, 2)])
    arrived(("r", 3), rb.at[1, pl.ds(2, 2)])
    arrived(("r", 4), rb.at[0, pl.ds(2, 2)])
    arrived(("r", 5), rb.at[1, pl.ds(0, 2)])
    mark("final")
    out_ref[...] = (mine + rb[0].astype(f32) + rb[1].astype(f32)).astype(bf16)

    mark("drain")
    left(0, tr.at[pl.ds(0, 3)])
    for m in range(4):
        left(1 + m, volume(m, 24))
    left(5, sm.at[pl.ds(0, 3)])
    left(6, hs)
    left(7, l1.at[pl.ds(0, 3)])
    left(8, pb)
    for d in range(1, 8):

        @pl.when(g + d < 8)
        def _():
            to_group(d).wait_send()

    assert len(slot.index) <= N_COPIES and len(local.index) <= N_LOCAL
    mark(None)


def per_device(
    tokens,
    norm_gain,
    entry_projection,
    valve_projection,
    filter_taps,
    conv_bias,
    recur_weight,
    recur_bias,
    entry_weight,
    entry_bias,
    forget_rate,
    output_weight,
):
    hbm = pl.BlockSpec(memory_space=pltpu.HBM)
    return pl.pallas_call(
        kernel,
        name="layer",
        out_shape=pltpu.VMEM((SEQS, TOK, D), bf16),
        in_specs=[hbm] * 12,
        out_specs=pl.BlockSpec(memory_space=pltpu.VMEM),
        scratch_shapes=[
            pltpu.VMEM((1, D), f32),
            pltpu.VMEM((SEQS, STR, D), bf16),
            pltpu.VMEM((ROWS, D), bf16),
            pltpu.VMEM((NB, AROWS, W), bf16),
            pltpu.VMEM((NB, D, W), bf16),
            pltpu.VMEM((NB, W, D), bf16),
            pltpu.VMEM((NB, 8, 1, W), f32),
            pltpu.VMEM((NB, ROWS, W), f32),
            pltpu.VMEM((NB, 32, W), bf16),
            pltpu.VMEM((NB, 32, W), bf16),
            pltpu.VMEM((ROWS, CH), bf16),
            pltpu.VMEM((2, ROWS, W), f32),
            pltpu.VMEM((NB, ROWS, W), f32),
            pltpu.VMEM((NB, ROWS, W), f32),
            pltpu.VMEM((NB, ROWS, W), f32),
            pltpu.VMEM((NB, ROWS, W), f32),
            pltpu.VMEM((ROWS, CH), bf16),
            pltpu.VMEM((8, CH), bf16),
            pltpu.VMEM((4, 8, CH), bf16),
            pltpu.VMEM((8, CH), bf16),
            pltpu.VMEM((8, 8, CH), bf16),
            pltpu.VMEM((3, SEQS, TOK, D), bf16),
            pltpu.VMEM((2, 2, TOK, D), f32),
            pltpu.VMEM((2, 2, TOK, D), bf16),
            pltpu.VMEM((2, SEQS, TOK, D), bf16),
            pltpu.SemaphoreType.DMA((N_SENDS,)),
            pltpu.SemaphoreType.DMA((N_COPIES,)),
            pltpu.SemaphoreType.DMA((N_LOCAL,)),
        ],
        compiler_params=pltpu.CompilerParams(
            collective_id=0, has_side_effects=True, vmem_limit_bytes=VMEM_LIMIT
        ),
    )(
        tokens,
        norm_gain.reshape(1, D),
        entry_projection,
        valve_projection,
        recur_weight,
        entry_weight,
        filter_taps.reshape(4, 1, W),
        conv_bias.reshape(1, W),
        recur_bias.reshape(1, W),
        entry_bias.reshape(1, W),
        forget_rate.reshape(1, W),
        output_weight,
    )


def solution(mesh):
    fine = Mesh(mesh.devices.reshape(4, 2, 4, 4), ("x", "c", "z", "y"))
    SP, TP = ("x", "c"), ("z", "y")
    both = SP + TP
    placed = (
        P(None, both, None),
        P(),
        P(None, TP),
        P(None, TP),
        P(None, TP),
        P(TP),
        P(TP, None, None),
        P(TP),
        P(TP, None, None),
        P(TP),
        P(TP),
        P(TP, None),
    )
    return jax.shard_map(
        per_device, mesh=fine, in_specs=placed, out_specs=P(None, both, None), check_vma=False
    )
```

```python
import jax
import jax.numpy as jnp
from jax import lax
from jax.experimental import pallas as pl
from jax.experimental.pallas import tpu as pltpu
from jax.sharding import Mesh
from jax.sharding import PartitionSpec as P

MESH = pl.DeviceIdType.MESH
EPS = 1e-06
POWER = 8.0
TINY = 1e-37
SEQS = 4
TOK = 16
STR = 64
D = 2048
W = 128
NB = 4
CH = NB * W
ROWS = SEQS * STR
AROWS = D + 2 * W
PIECE = ((AROWS // 16, 0), (AROWS // 16, AROWS // 2), (D // 8, 0), (W // 8, 0))
f32 = jnp.float32
bf16 = jnp.bfloat16


class Slots:
    def __init__(self):
        self.index = {}

    def __call__(self, *key):
        return self.index.setdefault(key, len(self.index))


N_COPIES = 44
N_SENDS = 16
N_LOCAL = 6
VMEM_LIMIT = 66700000


def neg_expm1(t):
    s = 1.0 + t * (1.0 / 8.0)
    for n in (7.0, 6.0, 5.0, 4.0, 3.0, 2.0):
        s = 1.0 + t * (1.0 / n) * s
    return jnp.where(t > -0.5, -t * s, 1.0 - jnp.exp(t))


def sigmoid(v):
    return 1.0 / (1.0 + jnp.exp(-v))


def kernel(
    tok_ref,
    gain_ref,
    w1_ref,
    w2_ref,
    rw_ref,
    ew_ref,
    taps_ref,
    cb_ref,
    rb_ref,
    eb_ref,
    rate_ref,
    wo_ref,
    out_ref,
    gain,
    tr,
    nt,
    wa,
    wv,
    wog,
    sm,
    ci,
    hs,
    hr,
    cv,
    lg,
    de,
    pu,
    sg,
    gt,
    g16,
    s_own,
    l1,
    t_own,
    l2,
    pb,
    pf,
    rd,
    rb,
    ssem,
    rsem,
    lsem,
):
    X = lax.axis_index("x")
    C = lax.axis_index("c")
    Z = lax.axis_index("z")
    Y = lax.axis_index("y")
    g = X * 2 + C
    par = lax.rem(X, 2)

    def mod4(v):
        return lax.rem(v + 8, 4)

    def gdev(v):
        return {"x": v // 2, "c": lax.rem(v, 2)}

    nxt_z = mod4(Z + 1)
    nxt_g = lax.rem(g + jnp.where(Z == 3, 1, 0), 8)
    prv_z = mod4(Z - 1)
    prv_g = lax.rem(g + 8 - jnp.where(Z == 0, 1, 0), 8)
    nxt = {"x": nxt_g // 2, "c": lax.rem(nxt_g, 2), "z": nxt_z}
    prv = {"x": prv_g // 2, "c": lax.rem(prv_g, 2), "z": prv_z}
    yp, ym = {"y": mod4(Y + 1)}, {"y": mod4(Y - 1)}
    zp, zm = {"z": nxt_z}, {"z": prv_z}
    xp, xm = {"x": mod4(X + 1)}, {"x": mod4(X - 1)}
    mate = {"c": 1 - C}

    slot = Slots()
    local = Slots()
    scopes = []

    def mark(name):
        if scopes:
            scopes.pop().__exit__(None, None, None)
        if name:
            scopes.append(jax.named_scope(name))
            scopes[-1].__enter__()

    def remote(out, key, src, dst, dev):
        return pltpu.make_async_remote_copy(
            src_ref=src,
            dst_ref=dst,
            send_sem=ssem.at[out],
            recv_sem=rsem.at[slot(*key)],
            device_id=dev,
            device_id_type=MESH,
        )

    def send(out, key, src, dst, dev):
        remote(out, key, src, dst, dev).start()

    def arrived(key, dst):
        remote(0, key, dst, dst, mate).wait_recv()

    def left(out, ref):
        remote(out, ("t", 0, 0), ref, ref, mate).wait_send()

    def fetch(key, src, dst):
        copy = pltpu.make_async_copy(src, dst, lsem.at[local(key)])
        copy.start()
        return copy

    mark("own")
    own_tok = tr.at[:, pl.ds(pl.multiple_of(Y * TOK, TOK), TOK), :]
    c_tok = fetch("tok", tok_ref, own_tok)
    fetch("wa", w1_ref, wa.at[Z, pl.ds(0, D)])
    fetch("wa", rw_ref.at[0], wa.at[Z, pl.ds(D, W)])
    fetch("wa", ew_ref.at[0], wa.at[Z, pl.ds(D + W, W)])
    fetch("sm", taps_ref, sm.at[Z, pl.ds(0, 4)])
    for n, ref in enumerate((cb_ref, rb_ref, eb_ref, rate_ref)):
        fetch("sm", ref, sm.at[Z, 4 + n])
    c_gain = fetch("gain", gain_ref, gain)
    c_wv = fetch("w2", w2_ref, wv.at[Z])
    c_wo = fetch("wo", wo_ref, wog.at[Z])

    l2[...] = jnp.zeros_like(l2)

    mark("barrier")
    barrier = pltpu.get_barrier_semaphore()
    partners = [yp, ym] + [{"z": mod4(Z + d)} for d in (1, 2, 3)]
    partners += [gdev(lax.rem(g + d, 8)) for d in range(1, 8)] + [nxt, prv]
    for dev in partners:
        pl.semaphore_signal(barrier, inc=1, device_id=dev, device_id_type=MESH)
    pl.semaphore_wait(barrier, len(partners))

    mark("tokens")
    def tok(y, half):
        return tr.at[pl.ds(2 * half, 2), pl.ds(pl.multiple_of(y * TOK, TOK), TOK), :]

    y_m, y_p, y_d = mod4(Y - 1), mod4(Y + 1), mod4(Y + 2)
    c_tok.wait()
    send(0, ("t", 0, 0), tok(Y, 0), tok(Y, 0), yp)
    send(0, ("t", 1, 1), tok(Y, 1), tok(Y, 1), ym)
    send(0, ("t", 0, 1), tok(Y, 1), tok(Y, 1), yp)
    send(0, ("t", 1, 0), tok(Y, 0), tok(Y, 0), ym)

    def piece(m, z, q, core, h):
        rows, base = PIECE[m]
        k = core * 2 + h
        if m == 1:
            rows = 2 * rows
        else:
            k = k + q * 4
        place = pl.ds(pl.multiple_of(base + k * rows, 16), rows)
        if m == 3:
            return wog.at[z, place]
        return (wa, wa, wv)[m].at[z, place]

    blocks = (mod4(Z - 1), mod4(Z + 1), mod4(Z + 2))

    def own_piece(m, j, h):
        ref = piece(m, Z, par, C, h)
        send(1 + m, ("z", m, j == h), ref, ref, zm if j else zp)

    def own_first(m):
        own_piece(m, 0, 0)
        own_piece(m, 1, 1)

    def own_second(m):
        own_piece(m, 0, 1)
        own_piece(m, 1, 0)

    def both(m):
        return (wa, wa, wv, wog)[m].at[0, pl.ds(0, PIECE[m][0] * (4 if m == 1 else 2))]

    def z_pair(m, pair, key):
        arrived(("z", m, key), both(m))
        for j, h in pair:
            ref = piece(m, blocks[j], par, C, h)
            if (j, h) == (0, 0):
                send(1 + m, ("z", m, 2), ref, ref, zp)
            if (j, h) == (1, 1):
                send(1 + m, ("z", m, 2), ref, ref, zm)
        for j, h in pair:
            ref = piece(m, blocks[j], par, C, h)
            if m != 1:
                send(1 + m, ("x", m, key), ref, ref, xp if h == 0 else xm)
            send(1 + m, ("d", m), ref, ref, mate)

    def x_pair(m, pair, key):
        arrived(("x", m, key), both(m))
        for j, h in pair:
            ref = piece(m, blocks[j], 1 - par, C, h)
            send(1 + m, ("d", m), ref, ref, mate)

    NEAR, NEXT, FAR = ((0, 0), (1, 1)), ((0, 1), (1, 0)), ((2, 0), (2, 1))

    def near_z(m):
        z_pair(m, NEAR, True)

    def next_z(m):
        z_pair(m, NEXT, False)

    def far_z(m):
        z_pair(m, FAR, 2)

    def near_x(m):
        x_pair(m, NEAR, True)

    def next_x(m):
        x_pair(m, NEXT, False)

    def far_x(m):
        x_pair(m, FAR, 2)

    def volume(m, parts):
        return (wa, wa, wv, wog)[m].at[pl.ds(0, parts // 6), pl.ds(0, PIECE[m][0] * 6)]

    mark("weights")
    pltpu.make_async_copy(wa.at[0], wa.at[0], lsem.at[local("wa")]).wait()
    own_first(0)
    own_second(0)
    own_first(1)
    pltpu.make_async_copy(sm.at[0], sm.at[0], lsem.at[local("sm")]).wait()
    for d in (1, 2, 3):
        send(5, ("s",), sm.at[Z], sm.at[Z], {"z": mod4(Z + d)})

    def norm(y, half):
        rows = pl.ds(pl.multiple_of(y * TOK, TOK), TOK)
        v = tr[pl.ds(2 * half, 2), rows, :].astype(f32)
        v = v * lax.rsqrt(jnp.mean(v * v, axis=-1, keepdims=True) + EPS)
        v = (v * gain[...].reshape(1, 1, D)).astype(bf16)
        for s in range(2):
            nt[pl.ds(pl.multiple_of((2 * half + s) * STR + y * TOK, TOK), TOK), :] = v[s]

    mark("norm0")
    c_gain.wait()
    norm(Y, 0)
    norm(Y, 1)
    mark("net0")
    near_z(0)
    own_second(1)
    mark("net1")
    next_z(0)
    mark("net1t")
    arrived(("t", 0, 0), tok(y_m, 0))
    send(0, ("t", 2, 0), tok(y_m, 0), tok(y_m, 0), yp)
    arrived(("t", 1, 1), tok(y_p, 1))
    send(0, ("t", 2, 1), tok(y_p, 1), tok(y_p, 1), ym)
    mark("net2")
    near_z(1)
    c_wv.wait()
    own_first(2)
    own_second(2)
    c_wo.wait()
    own_first(3)
    own_second(3)
    mark("norm1")
    norm(y_m, 0)
    norm(y_p, 1)
    mark("net3")
    far_z(0)
    mark("net3a")
    near_x(0)
    next_x(0)
    mark("net3b")
    next_z(1)
    mark("net3t")
    arrived(("t", 0, 1), tok(y_m, 1))
    arrived(("t", 1, 0), tok(y_p, 0))
    mark("norm2")
    norm(y_m, 1)
    norm(y_p, 0)
    mark("net4")
    far_z(1)
    mark("net5")
    far_x(0)
    mark("net5t")
    arrived(("t", 2, 0), tok(y_d, 0))
    norm(y_d, 0)
    arrived(("t", 2, 1), tok(y_d, 1))
    norm(y_d, 1)
    mark("d0")
    arrived(("d", 0), volume(0, 12))
    arrived(("d", 1), volume(1, 12))

    mark("matmul1")

    def pair(ref, b):
        rhs = jnp.concatenate([ref[b, 0:D, :], ref[b + 1, 0:D, :]], axis=1)
        return jnp.dot(nt[...], rhs, preferred_element_type=f32).astype(bf16).astype(f32)

    for b in range(0, NB, 2):
        part = pair(wa, b)
        ci[b] = part[:, 0:W]
        ci[b + 1] = part[:, W : 2 * W]
        for n in (b, b + 1):
            for s in range(SEQS):
                last = part[s * STR + STR - 8 : s * STR + STR, (n - b) * W : (n - b + 1) * W]
                hs[n, s * 8 : s * 8 + 8, :] = last.astype(bf16)
    send(6, ("h",), hs, hr, nxt)
    mark("net6")
    near_z(2)
    arrived(("s",), sm.at[pl.ds(0, 3)])

    mark("conv")
    lane_row = lax.broadcasted_iota(jnp.int32, (8, W), 0)

    def convolve(b, at):
        acc = jnp.broadcast_to(sm[b, 4], (8, W))
        for k in range(4):
            acc = acc + at(k - 3) * sm[b, k]
        return acc

    for b in range(NB):
        for s in range(SEQS):
            x = [ci[b, pl.ds(s * STR + i, 8, stride=8), :] for i in range(8)]
            prev = {i - 8: pltpu.roll(x[i], 1, 0) for i in (5, 6, 7)}
            rows = []
            for i in range(8):
                rows.append(convolve(b, lambda n: x[i + n] if i + n >= 0 else prev[i + n]))
            cv[pl.ds(s * STR, STR), b * W : (b + 1) * W] = jnp.concatenate(rows, axis=0).astype(bf16)

    mark("gates")

    def gates(b, logit_r, logit_e, conv):
        r_gate = sigmoid(logit_r + sm[b, 5])
        e_gate = sigmoid(logit_e + sm[b, 6])
        log_decay = (-POWER * r_gate) * sm[b, 7]
        push = jnp.sqrt(neg_expm1(2.0 * log_decay)) * (e_gate * conv.astype(f32))
        return jnp.exp(log_decay), push

    def gate_dots(b, conv):
        return [
            jnp.dot(conv, wa[b, D + n * W : D + (n + 1) * W, :], preferred_element_type=f32)
            for n in range(2)
        ]

    for b in range(NB):
        cols = slice(b * W, (b + 1) * W)
        lg[0], lg[1] = gate_dots(b, cv[:, cols])
        for s in range(SEQS):
            rows = slice(s * STR, (s + 1) * STR)
            de[b, rows, :], pu[b, rows, :] = gates(b, lg[0, rows, :], lg[1, rows, :], cv[rows, cols])

    mark("net7")
    next_z(2)
    near_z(3)
    mark("halo")
    arrived(("h",), hr)
    mark("redo")
    start = jnp.logical_and(g == 0, Z == 0)
    for b in range(NB):
        tiles = []
        for s in range(SEQS):
            behind = jnp.where(start, 0.0, hr[b, s * 8 : s * 8 + 8, :].astype(f32))
            here = ci[b, s * STR : s * STR + 8, :]

            def at(n):
                if n == 0:
                    return here
                return jnp.where(lane_row < -n, pltpu.roll(behind, -n, 0), pltpu.roll(here, -n, 0))

            tiles.append(convolve(b, at))
        conv = jnp.concatenate(tiles, axis=0).astype(bf16)
        decay, push = gates(b, *gate_dots(b, conv), conv)
        for s in range(SEQS):
            chain = pl.ds(s * STR, 8, stride=8)
            de[b, chain, :] = decay[s * 8 : s * 8 + 8]
            pu[b, chain, :] = push[s * 8 : s * 8 + 8]

    mark("scan")
    ends = [[None] * SEQS for _ in range(NB)]
    for b in range(NB):
        cols = slice(b * W, (b + 1) * W)
        tot_a, tot_h = [], []
        for s in range(SEQS):
            a = de[b, s * STR : s * STR + 8, :]
            h = pu[b, s * STR : s * STR + 8, :]
            for i in range(1, 8):
                at = slice(s * STR + i * 8, s * STR + i * 8 + 8)
                step = de[b, at, :]
                h = step * h + pu[b, at, :]
                a = step * a
                de[b, at, :] = a
                pu[b, at, :] = h
            for n in (1, 2, 4):
                keep = lane_row >= n
                a_in = jnp.where(keep, pltpu.roll(a, n, 0), 1.0)
                h_in = jnp.where(keep, pltpu.roll(h, n, 0), 0.0)
                h = a * h_in + h
                a = a * a_in
            tot_a.append(a[7:8])
            tot_h.append(h[7:8])
            ends[b][s] = (
                jnp.where(lane_row >= 1, pltpu.roll(a, 1, 0), 1.0),
                jnp.where(lane_row >= 1, pltpu.roll(h, 1, 0), 0.0),
            )
        tot_a = [jnp.log(jnp.maximum(a, TINY)) for a in tot_a]
        s_own[:, cols] = jnp.concatenate(tot_a + tot_h, axis=0).astype(bf16)

    mark("states")
    for d in (2, 1, 3):
        send(7, ("e",), s_own, l1.at[Z], {"z": mod4(Z + d)})
    l1[Z] = s_own[...]
    near_x(2)
    next_z(3)
    far_z(2)
    next_x(2)
    near_x(3)
    far_z(3)
    mark("states1")
    arrived(("e",), l1.at[pl.ds(0, 3)])
    total_a, total_h = l1[0, 0:4].astype(f32), l1[0, 4:8].astype(f32)
    for k in range(1, 4):
        ka, kh = l1[k, 0:4].astype(f32), l1[k, 4:8].astype(f32)
        total_h = jnp.exp(ka) * total_h + kh
        total_a = ka + total_a
    t_own[...] = jnp.concatenate([total_a, total_h], axis=0).astype(bf16)

    def to_group(d):
        return remote(8 + d, ("g", d), t_own, l2.at[g], gdev(lax.rem(g + d, 8)))

    for d in (4, 5, 3, 2, 6, 7, 1):

        @pl.when(g + d < 8)
        def _():
            to_group(d).start()

    mark("net8")
    far_x(2)
    mark("net8d")
    arrived(("d", 2), volume(2, 12))
    mark("valve")
    for b in range(0, NB, 2):
        v = pair(wv, b)
        v = v / (1.0 + jnp.exp(-v))
        sg[b] = v[:, 0:W]
        sg[b + 1] = v[:, W : 2 * W]
    mark("net9")
    next_x(3)
    far_x(3)
    mark("states2")
    for d in range(1, 8):

        @pl.when(g - d >= 0)
        def _():
            arrived(("g", d), l2.at[lax.rem(g - d + 8, 8)])

    mark("entering")
    state = jnp.zeros((SEQS, CH), f32)
    for k in range(7):
        state = jnp.where(k < g, jnp.exp(l2[k, 0:4].astype(f32)) * state + l2[k, 4:8].astype(f32), state)
    for k in range(3):
        state = jnp.where(k < Z, jnp.exp(l1[k, 0:4].astype(f32)) * state + l1[k, 4:8].astype(f32), state)

    mark("gated")
    for b in range(NB):
        cols = slice(b * W, (b + 1) * W)
        for s in range(SEQS):
            chain_a, chain_h = ends[b][s]
            enter = chain_a * jnp.broadcast_to(state[s : s + 1, cols], (8, W)) + chain_h
            for i in range(8):
                at = s * STR + i * 8
                h = de[b, at : at + 8, :] * enter + pu[b, at : at + 8, :]
                places = pl.ds(s * STR + i, 8, stride=8)
                gt[b, places, :] = h * sg[b, places, :]
        g16[:, cols] = gt[b].astype(bf16)

    mark("d2")
    arrived(("d", 3), volume(3, 12))

    def product(y):
        lhs = jnp.concatenate(
            [g16[pl.ds(pl.multiple_of(s * STR + y * TOK, TOK), TOK), :] for s in range(SEQS)], axis=0
        )
        return jnp.dot(lhs, wog[...].reshape(CH, D), preferred_element_type=f32)

    mark("prod0")
    p = product(y_d).astype(bf16).reshape(SEQS, TOK, D)
    pb[0] = p
    send(8, ("r", 0), pb.at[0, pl.ds(0, 2)], rd.at[0], ym)
    send(8, ("r", 1), pb.at[0, pl.ds(2, 2)], rd.at[1], yp)
    mark("prod1")
    p = product(y_p).reshape(SEQS, TOK, D)
    pb[1, 0:2] = p[0:2].astype(bf16)
    send(8, ("r", 2), pb.at[1, pl.ds(0, 2)], rb.at[0, pl.ds(0, 2)], yp)
    pf[1] = p[2:4]
    p = product(y_m).reshape(SEQS, TOK, D)
    pb[2, 2:4] = p[2:4].astype(bf16)
    send(8, ("r", 2), pb.at[2, pl.ds(2, 2)], rb.at[1, pl.ds(2, 2)], ym)
    pf[0] = p[0:2]
    mine = product(Y).reshape(SEQS, TOK, D)
    mark("red1")
    arrived(("r", 1), rd.at[1])
    pb[1, 2:4] = (pf[1] + rd[1].astype(f32)).astype(bf16)
    send(8, ("r", 2), pb.at[1, pl.ds(2, 2)], rb.at[0, pl.ds(2, 2)], yp)
    arrived(("r", 0), rd.at[0])
    pb[2, 0:2] = (pf[0] + rd[0].astype(f32)).astype(bf16)
    send(8, ("r", 2), pb.at[2, pl.ds(0, 2)], rb.at[1, pl.ds(0, 2)], ym)
    mark("red2")
    arrived(("r", 2), rb)
    mark("final")
    out_ref[...] = (mine + rb[0].astype(f32) + rb[1].astype(f32)).astype(bf16)

    mark("drain")
    left(0, tr.at[pl.ds(0, 3)])
    for m in range(4):
        left(1 + m, volume(m, 24))
    left(5, sm.at[pl.ds(0, 3)])
    left(6, hs)
    left(7, l1.at[pl.ds(0, 3)])
    left(8, pb)
    for d in range(1, 8):

        @pl.when(g + d < 8)
        def _():
            to_group(d).wait_send()

    assert len(slot.index) == N_COPIES and len(local.index) == N_LOCAL
    mark(None)


def per_device(
    tokens,
    norm_gain,
    entry_projection,
    valve_projection,
    filter_taps,
    conv_bias,
    recur_weight,
    recur_bias,
    entry_weight,
    entry_bias,
    forget_rate,
    output_weight,
):
    hbm = pl.BlockSpec(memory_space=pltpu.HBM)
    return pl.pallas_call(
        kernel,
        name="layer",
        out_shape=pltpu.VMEM((SEQS, TOK, D), bf16),
        in_specs=[hbm] * 12,
        out_specs=pl.BlockSpec(memory_space=pltpu.VMEM),
        scratch_shapes=[
            pltpu.VMEM((1, D), f32),
            pltpu.VMEM((SEQS, STR, D), bf16),
            pltpu.VMEM((ROWS, D), bf16),
            pltpu.VMEM((NB, AROWS, W), bf16),
            pltpu.VMEM((NB, D, W), bf16),
            pltpu.VMEM((NB, W, D), bf16),
            pltpu.VMEM((NB, 8, 1, W), f32),
            pltpu.VMEM((NB, ROWS, W), f32),
            pltpu.VMEM((NB, 32, W), bf16),
            pltpu.VMEM((NB, 32, W), bf16),
            pltpu.VMEM((ROWS, CH), bf16),
            pltpu.VMEM((2, ROWS, W), f32),
            pltpu.VMEM((NB, ROWS, W), f32),
            pltpu.VMEM((NB, ROWS, W), f32),
            pltpu.VMEM((NB, ROWS, W), f32),
            pltpu.VMEM((NB, ROWS, W), f32),
            pltpu.VMEM((ROWS, CH), bf16),
            pltpu.VMEM((8, CH), bf16),
            pltpu.VMEM((4, 8, CH), bf16),
            pltpu.VMEM((8, CH), bf16),
            pltpu.VMEM((8, 8, CH), bf16),
            pltpu.VMEM((3, SEQS, TOK, D), bf16),
            pltpu.VMEM((2, 2, TOK, D), f32),
            pltpu.VMEM((2, 2, TOK, D), bf16),
            pltpu.VMEM((2, SEQS, TOK, D), bf16),
            pltpu.SemaphoreType.DMA((N_SENDS,)),
            pltpu.SemaphoreType.DMA((N_COPIES,)),
            pltpu.SemaphoreType.DMA((N_LOCAL,)),
        ],
        compiler_params=pltpu.CompilerParams(
            collective_id=0, has_side_effects=True, vmem_limit_bytes=VMEM_LIMIT
        ),
    )(
        tokens,
        norm_gain.reshape(1, D),
        entry_projection,
        valve_projection,
        recur_weight,
        entry_weight,
        filter_taps.reshape(4, 1, W),
        conv_bias.reshape(1, W),
        recur_bias.reshape(1, W),
        entry_bias.reshape(1, W),
        forget_rate.reshape(1, W),
        output_weight,
    )


def solution(mesh):
    fine = Mesh(mesh.devices.reshape(4, 2, 4, 4), ("x", "c", "z", "y"))
    SP, TP = ("x", "c"), ("z", "y")
    both = SP + TP
    placed = (
        P(None, both, None),
        P(),
        P(None, TP),
        P(None, TP),
        P(None, TP),
        P(TP),
        P(TP, None, None),
        P(TP),
        P(TP, None, None),
        P(TP),
        P(TP),
        P(TP, None),
    )
    return jax.shard_map(
        per_device, mesh=fine, in_specs=placed, out_specs=P(None, both, None), check_vma=False
    )
```

```python
import jax
import jax.numpy as jnp
from jax import lax
from jax.experimental import pallas as pl
from jax.experimental.pallas import tpu as pltpu
from jax.sharding import Mesh
from jax.sharding import PartitionSpec as P

MESH = pl.DeviceIdType.MESH
EPS = 1e-06
POWER = 8.0
TINY = 1e-37
SEQS = 4
TOK = 16
STR = 64
D = 2048
W = 128
NB = 4
CH = NB * W
ROWS = SEQS * STR
AROWS = D + 2 * W
PIECE = ((AROWS // 12, 0), (AROWS // 24, AROWS * 2 // 3), (D // 8, 0), (W // 8, 0))
f32 = jnp.float32
bf16 = jnp.bfloat16


class Slots:
    def __init__(self):
        self.index = {}

    def __call__(self, *key):
        return self.index.setdefault(key, len(self.index))


N_COPIES = 44
N_SENDS = 16
N_LOCAL = 6
VMEM_LIMIT = 66700000


def neg_expm1(t):
    s = 1.0 + t * (1.0 / 8.0)
    for n in (7.0, 6.0, 5.0, 4.0, 3.0, 2.0):
        s = 1.0 + t * (1.0 / n) * s
    return jnp.where(t > -0.5, -t * s, 1.0 - jnp.exp(t))


def sigmoid(v):
    return 1.0 / (1.0 + jnp.exp(-v))


def kernel(
    tok_ref,
    gain_ref,
    w1_ref,
    w2_ref,
    rw_ref,
    ew_ref,
    taps_ref,
    cb_ref,
    rb_ref,
    eb_ref,
    rate_ref,
    wo_ref,
    out_ref,
    gain,
    tr,
    nt,
    wa,
    wv,
    wog,
    sm,
    ci,
    hs,
    hr,
    cv,
    lg,
    de,
    pu,
    sg,
    gt,
    g16,
    s_own,
    l1,
    t_own,
    l2,
    pb,
    pf,
    rd,
    rb,
    ssem,
    rsem,
    lsem,
):
    X = lax.axis_index("x")
    C = lax.axis_index("c")
    Z = lax.axis_index("z")
    Y = lax.axis_index("y")
    g = X * 2 + C
    par = lax.rem(X, 2)

    def mod4(v):
        return lax.rem(v + 8, 4)

    def gdev(v):
        return {"x": v // 2, "c": lax.rem(v, 2)}

    nxt_z = mod4(Z + 1)
    nxt_g = lax.rem(g + jnp.where(Z == 3, 1, 0), 8)
    prv_z = mod4(Z - 1)
    prv_g = lax.rem(g + 8 - jnp.where(Z == 0, 1, 0), 8)
    nxt = {"x": nxt_g // 2, "c": lax.rem(nxt_g, 2), "z": nxt_z}
    prv = {"x": prv_g // 2, "c": lax.rem(prv_g, 2), "z": prv_z}
    yp, ym = {"y": mod4(Y + 1)}, {"y": mod4(Y - 1)}
    zp, zm = {"z": nxt_z}, {"z": prv_z}
    xp, xm = {"x": mod4(X + 1)}, {"x": mod4(X - 1)}
    mate = {"c": 1 - C}

    slot = Slots()
    local = Slots()
    scopes = []

    def mark(name):
        if scopes:
            scopes.pop().__exit__(None, None, None)
        if name:
            scopes.append(jax.named_scope(name))
            scopes[-1].__enter__()

    def remote(out, key, src, dst, dev):
        return pltpu.make_async_remote_copy(
            src_ref=src,
            dst_ref=dst,
            send_sem=ssem.at[out],
            recv_sem=rsem.at[slot(*key)],
            device_id=dev,
            device_id_type=MESH,
        )

    def send(out, key, src, dst, dev):
        remote(out, key, src, dst, dev).start()

    def arrived(key, dst):
        remote(0, key, dst, dst, mate).wait_recv()

    def left(out, ref):
        remote(out, ("t", 0, 0), ref, ref, mate).wait_send()

    def fetch(key, src, dst):
        copy = pltpu.make_async_copy(src, dst, lsem.at[local(key)])
        copy.start()
        return copy

    mark("own")
    own_tok = tr.at[:, pl.ds(pl.multiple_of(Y * TOK, TOK), TOK), :]
    c_tok = fetch("tok", tok_ref, own_tok)
    fetch("wa", w1_ref, wa.at[Z, pl.ds(0, D)])
    fetch("wa", rw_ref.at[0], wa.at[Z, pl.ds(D, W)])
    fetch("wa", ew_ref.at[0], wa.at[Z, pl.ds(D + W, W)])
    fetch("sm", taps_ref, sm.at[Z, pl.ds(0, 4)])
    for n, ref in enumerate((cb_ref, rb_ref, eb_ref, rate_ref)):
        fetch("sm", ref, sm.at[Z, 4 + n])
    c_gain = fetch("gain", gain_ref, gain)
    c_wv = fetch("w2", w2_ref, wv.at[Z])
    c_wo = fetch("wo", wo_ref, wog.at[Z])

    l2[...] = jnp.zeros_like(l2)

    mark("barrier")
    barrier = pltpu.get_barrier_semaphore()
    partners = [yp, ym] + [{"z": mod4(Z + d)} for d in (1, 2, 3)]
    partners += [gdev(lax.rem(g + d, 8)) for d in range(1, 8)] + [nxt, prv]
    for dev in partners:
        pl.semaphore_signal(barrier, inc=1, device_id=dev, device_id_type=MESH)
    pl.semaphore_wait(barrier, len(partners))

    mark("tokens")
    def tok(y, half):
        return tr.at[pl.ds(2 * half, 2), pl.ds(pl.multiple_of(y * TOK, TOK), TOK), :]

    y_m, y_p, y_d = mod4(Y - 1), mod4(Y + 1), mod4(Y + 2)
    c_tok.wait()
    send(0, ("t", 0, 0), tok(Y, 0), tok(Y, 0), yp)
    send(0, ("t", 1, 1), tok(Y, 1), tok(Y, 1), ym)
    send(0, ("t", 0, 1), tok(Y, 1), tok(Y, 1), yp)
    send(0, ("t", 1, 0), tok(Y, 0), tok(Y, 0), ym)

    def piece(m, z, q, core, h):
        rows, base = PIECE[m]
        k = core * 2 + h
        if m == 1:
            rows = 2 * rows
        else:
            k = k + q * 4
        place = pl.ds(pl.multiple_of(base + k * rows, 16), rows)
        if m == 3:
            return wog.at[z, place]
        return (wa, wa, wv)[m].at[z, place]

    blocks = (mod4(Z - 1), mod4(Z + 1), mod4(Z + 2))

    def own_piece(m, j, h):
        ref = piece(m, Z, par, C, h)
        send(1 + m, ("z", m, j == h), ref, ref, zm if j else zp)

    def own_first(m):
        own_piece(m, 0, 0)
        own_piece(m, 1, 1)

    def own_second(m):
        own_piece(m, 0, 1)
        own_piece(m, 1, 0)

    def both(m):
        return (wa, wa, wv, wog)[m].at[0, pl.ds(0, PIECE[m][0] * (4 if m == 1 else 2))]

    def z_pair(m, pair, key):
        arrived(("z", m, key), both(m))
        for j, h in pair:
            ref = piece(m, blocks[j], par, C, h)
            if (j, h) == (0, 0):
                send(1 + m, ("z", m, 2), ref, ref, zp)
            if (j, h) == (1, 1):
                send(1 + m, ("z", m, 2), ref, ref, zm)
        for j, h in pair:
            ref = piece(m, blocks[j], par, C, h)
            if m != 1:
                send(1 + m, ("x", m, key), ref, ref, xp if h == 0 else xm)
            send(1 + m, ("d", m), ref, ref, mate)

    def x_pair(m, pair, key):
        arrived(("x", m, key), both(m))
        for j, h in pair:
            ref = piece(m, blocks[j], 1 - par, C, h)
            send(1 + m, ("d", m), ref, ref, mate)

    NEAR, NEXT, FAR = ((0, 0), (1, 1)), ((0, 1), (1, 0)), ((2, 0), (2, 1))

    def near_z(m):
        z_pair(m, NEAR, True)

    def next_z(m):
        z_pair(m, NEXT, False)

    def far_z(m):
        z_pair(m, FAR, 2)

    def near_x(m):
        x_pair(m, NEAR, True)

    def next_x(m):
        x_pair(m, NEXT, False)

    def far_x(m):
        x_pair(m, FAR, 2)

    def volume(m, parts):
        return (wa, wa, wv, wog)[m].at[pl.ds(0, parts // 6), pl.ds(0, PIECE[m][0] * 6)]

    mark("weights")
    pltpu.make_async_copy(wa.at[0], wa.at[0], lsem.at[local("wa")]).wait()
    own_first(0)
    own_second(0)
    own_first(1)
    pltpu.make_async_copy(sm.at[0], sm.at[0], lsem.at[local("sm")]).wait()
    for d in (1, 2, 3):
        send(5, ("s",), sm.at[Z], sm.at[Z], {"z": mod4(Z + d)})

    def norm(y, half):
        rows = pl.ds(pl.multiple_of(y * TOK, TOK), TOK)
        v = tr[pl.ds(2 * half, 2), rows, :].astype(f32)
        v = v * lax.rsqrt(jnp.mean(v * v, axis=-1, keepdims=True) + EPS)
        v = (v * gain[...].reshape(1, 1, D)).astype(bf16)
        for s in range(2):
            nt[pl.ds(pl.multiple_of((2 * half + s) * STR + y * TOK, TOK), TOK), :] = v[s]

    mark("norm0")
    c_gain.wait()
    norm(Y, 0)
    norm(Y, 1)
    mark("net0")
    near_z(0)
    own_second(1)
    mark("net1")
    next_z(0)
    mark("net1t")
    arrived(("t", 0, 0), tok(y_m, 0))
    send(0, ("t", 2, 0), tok(y_m, 0), tok(y_m, 0), yp)
    arrived(("t", 1, 1), tok(y_p, 1))
    send(0, ("t", 2, 1), tok(y_p, 1), tok(y_p, 1), ym)
    mark("net2")
    near_z(1)
    c_wv.wait()
    own_first(2)
    own_second(2)
    c_wo.wait()
    own_first(3)
    own_second(3)
    mark("norm1")
    norm(y_m, 0)
    norm(y_p, 1)
    mark("net3")
    far_z(0)
    mark("net3a")
    near_x(0)
    next_x(0)
    mark("net3b")
    next_z(1)
    mark("net3t")
    arrived(("t", 0, 1), tok(y_m, 1))
    arrived(("t", 1, 0), tok(y_p, 0))
    mark("norm2")
    norm(y_m, 1)
    norm(y_p, 0)
    mark("net4")
    far_z(1)
    mark("net5")
    far_x(0)
    mark("net5t")
    arrived(("t", 2, 0), tok(y_d, 0))
    norm(y_d, 0)
    arrived(("t", 2, 1), tok(y_d, 1))
    norm(y_d, 1)
    mark("d0")
    arrived(("d", 0), volume(0, 12))
    arrived(("d", 1), volume(1, 12))

    mark("matmul1")

    def pair(ref, b):
        rhs = jnp.concatenate([ref[b, 0:D, :], ref[b + 1, 0:D, :]], axis=1)
        return jnp.dot(nt[...], rhs, preferred_element_type=f32).astype(bf16).astype(f32)

    for b in range(0, NB, 2):
        part = pair(wa, b)
        ci[b] = part[:, 0:W]
        ci[b + 1] = part[:, W : 2 * W]
        for n in (b, b + 1):
            for s in range(SEQS):
                last = part[s * STR + STR - 8 : s * STR + STR, (n - b) * W : (n - b + 1) * W]
                hs[n, s * 8 : s * 8 + 8, :] = last.astype(bf16)
    send(6, ("h",), hs, hr, nxt)
    mark("net6")
    near_z(2)
    arrived(("s",), sm.at[pl.ds(0, 3)])

    mark("conv")
    lane_row = lax.broadcasted_iota(jnp.int32, (8, W), 0)

    def convolve(b, at):
        acc = jnp.broadcast_to(sm[b, 4], (8, W))
        for k in range(4):
            acc = acc + at(k - 3) * sm[b, k]
        return acc

    for b in range(NB):
        for s in range(SEQS):
            x = [ci[b, pl.ds(s * STR + i, 8, stride=8), :] for i in range(8)]
            prev = {i - 8: pltpu.roll(x[i], 1, 0) for i in (5, 6, 7)}
            rows = []
            for i in range(8):
                rows.append(convolve(b, lambda n: x[i + n] if i + n >= 0 else prev[i + n]))
            cv[pl.ds(s * STR, STR), b * W : (b + 1) * W] = jnp.concatenate(rows, axis=0).astype(bf16)

    mark("gates")

    def gates(b, logit_r, logit_e, conv):
        r_gate = sigmoid(logit_r + sm[b, 5])
        e_gate = sigmoid(logit_e + sm[b, 6])
        log_decay = (-POWER * r_gate) * sm[b, 7]
        push = jnp.sqrt(neg_expm1(2.0 * log_decay)) * (e_gate * conv.astype(f32))
        return jnp.exp(log_decay), push

    def gate_dots(b, conv):
        return [
            jnp.dot(conv, wa[b, D + n * W : D + (n + 1) * W, :], preferred_element_type=f32)
            for n in range(2)
        ]

    for b in range(NB):
        cols = slice(b * W, (b + 1) * W)
        lg[0], lg[1] = gate_dots(b, cv[:, cols])
        for s in range(SEQS):
            rows = slice(s * STR, (s + 1) * STR)
            de[b, rows, :], pu[b, rows, :] = gates(b, lg[0, rows, :], lg[1, rows, :], cv[rows, cols])

    mark("net7")
    next_z(2)
    near_z(3)
    mark("halo")
    arrived(("h",), hr)
    mark("redo")
    start = jnp.logical_and(g == 0, Z == 0)
    for b in range(NB):
        tiles = []
        for s in range(SEQS):
            behind = jnp.where(start, 0.0, hr[b, s * 8 : s * 8 + 8, :].astype(f32))
            here = ci[b, s * STR : s * STR + 8, :]

            def at(n):
                if n == 0:
                    return here
                return jnp.where(lane_row < -n, pltpu.roll(behind, -n, 0), pltpu.roll(here, -n, 0))

            tiles.append(convolve(b, at))
        conv = jnp.concatenate(tiles, axis=0).astype(bf16)
        decay, push = gates(b, *gate_dots(b, conv), conv)
        for s in range(SEQS):
            chain = pl.ds(s * STR, 8, stride=8)
            de[b, chain, :] = decay[s * 8 : s * 8 + 8]
            pu[b, chain, :] = push[s * 8 : s * 8 + 8]

    mark("scan")
    ends = [[None] * SEQS for _ in range(NB)]
    for b in range(NB):
        cols = slice(b * W, (b + 1) * W)
        tot_a, tot_h = [], []
        for s in range(SEQS):
            a = de[b, s * STR : s * STR + 8, :]
            h = pu[b, s * STR : s * STR + 8, :]
            for i in range(1, 8):
                at = slice(s * STR + i * 8, s * STR + i * 8 + 8)
                step = de[b, at, :]
                h = step * h + pu[b, at, :]
                a = step * a
                de[b, at, :] = a
                pu[b, at, :] = h
            for n in (1, 2, 4):
                keep = lane_row >= n
                a_in = jnp.where(keep, pltpu.roll(a, n, 0), 1.0)
                h_in = jnp.where(keep, pltpu.roll(h, n, 0), 0.0)
                h = a * h_in + h
                a = a * a_in
            tot_a.append(a[7:8])
            tot_h.append(h[7:8])
            ends[b][s] = (
                jnp.where(lane_row >= 1, pltpu.roll(a, 1, 0), 1.0),
                jnp.where(lane_row >= 1, pltpu.roll(h, 1, 0), 0.0),
            )
        tot_a = [jnp.log(jnp.maximum(a, TINY)) for a in tot_a]
        s_own[:, cols] = jnp.concatenate(tot_a + tot_h, axis=0).astype(bf16)

    mark("states")
    for d in (2, 1, 3):
        send(7, ("e",), s_own, l1.at[Z], {"z": mod4(Z + d)})
    l1[Z] = s_own[...]
    near_x(2)
    next_z(3)
    far_z(2)
    next_x(2)
    near_x(3)
    far_z(3)
    mark("states1")
    arrived(("e",), l1.at[pl.ds(0, 3)])
    total_a, total_h = l1[0, 0:4].astype(f32), l1[0, 4:8].astype(f32)
    for k in range(1, 4):
        ka, kh = l1[k, 0:4].astype(f32), l1[k, 4:8].astype(f32)
        total_h = jnp.exp(ka) * total_h + kh
        total_a = ka + total_a
    t_own[...] = jnp.concatenate([total_a, total_h], axis=0).astype(bf16)

    def to_group(d):
        return remote(8 + d, ("g", d), t_own, l2.at[g], gdev(lax.rem(g + d, 8)))

    for d in (4, 5, 3, 2, 6, 7, 1):

        @pl.when(g + d < 8)
        def _():
            to_group(d).start()

    mark("net8")
    far_x(2)
    mark("net8d")
    arrived(("d", 2), volume(2, 12))
    mark("valve")
    for b in range(0, NB, 2):
        v = pair(wv, b)
        v = v / (1.0 + jnp.exp(-v))
        sg[b] = v[:, 0:W]
        sg[b + 1] = v[:, W : 2 * W]
    mark("net9")
    next_x(3)
    far_x(3)
    mark("states2")
    for d in range(1, 8):

        @pl.when(g - d >= 0)
        def _():
            arrived(("g", d), l2.at[lax.rem(g - d + 8, 8)])

    mark("entering")
    state = jnp.zeros((SEQS, CH), f32)
    for k in range(7):
        state = jnp.where(k < g, jnp.exp(l2[k, 0:4].astype(f32)) * state + l2[k, 4:8].astype(f32), state)
    for k in range(3):
        state = jnp.where(k < Z, jnp.exp(l1[k, 0:4].astype(f32)) * state + l1[k, 4:8].astype(f32), state)

    mark("gated")
    for b in range(NB):
        cols = slice(b * W, (b + 1) * W)
        for s in range(SEQS):
            chain_a, chain_h = ends[b][s]
            enter = chain_a * jnp.broadcast_to(state[s : s + 1, cols], (8, W)) + chain_h
            for i in range(8):
                at = s * STR + i * 8
                h = de[b, at : at + 8, :] * enter + pu[b, at : at + 8, :]
                places = pl.ds(s * STR + i, 8, stride=8)
                gt[b, places, :] = h * sg[b, places, :]
        g16[:, cols] = gt[b].astype(bf16)

    mark("d2")
    arrived(("d", 3), volume(3, 12))

    def product(y):
        lhs = jnp.concatenate(
            [g16[pl.ds(pl.multiple_of(s * STR + y * TOK, TOK), TOK), :] for s in range(SEQS)], axis=0
        )
        return jnp.dot(lhs, wog[...].reshape(CH, D), preferred_element_type=f32)

    mark("prod0")
    p = product(y_d).astype(bf16).reshape(SEQS, TOK, D)
    pb[0] = p
    send(8, ("r", 0), pb.at[0, pl.ds(0, 2)], rd.at[0], ym)
    send(8, ("r", 1), pb.at[0, pl.ds(2, 2)], rd.at[1], yp)
    mark("prod1")
    p = product(y_p).reshape(SEQS, TOK, D)
    pb[1, 0:2] = p[0:2].astype(bf16)
    send(8, ("r", 2), pb.at[1, pl.ds(0, 2)], rb.at[0, pl.ds(0, 2)], yp)
    pf[1] = p[2:4]
    p = product(y_m).reshape(SEQS, TOK, D)
    pb[2, 2:4] = p[2:4].astype(bf16)
    send(8, ("r", 2), pb.at[2, pl.ds(2, 2)], rb.at[1, pl.ds(2, 2)], ym)
    pf[0] = p[0:2]
    mine = product(Y).reshape(SEQS, TOK, D)
    mark("red1")
    arrived(("r", 1), rd.at[1])
    pb[1, 2:4] = (pf[1] + rd[1].astype(f32)).astype(bf16)
    send(8, ("r", 2), pb.at[1, pl.ds(2, 2)], rb.at[0, pl.ds(2, 2)], yp)
    arrived(("r", 0), rd.at[0])
    pb[2, 0:2] = (pf[0] + rd[0].astype(f32)).astype(bf16)
    send(8, ("r", 2), pb.at[2, pl.ds(0, 2)], rb.at[1, pl.ds(0, 2)], ym)
    mark("red2")
    arrived(("r", 2), rb)
    mark("final")
    out_ref[...] = (mine + rb[0].astype(f32) + rb[1].astype(f32)).astype(bf16)

    mark("drain")
    left(0, tr.at[pl.ds(0, 3)])
    for m in range(4):
        left(1 + m, volume(m, 24))
    left(5, sm.at[pl.ds(0, 3)])
    left(6, hs)
    left(7, l1.at[pl.ds(0, 3)])
    left(8, pb)
    for d in range(1, 8):

        @pl.when(g + d < 8)
        def _():
            to_group(d).wait_send()

    assert len(slot.index) == N_COPIES and len(local.index) == N_LOCAL
    mark(None)


def per_device(
    tokens,
    norm_gain,
    entry_projection,
    valve_projection,
    filter_taps,
    conv_bias,
    recur_weight,
    recur_bias,
    entry_weight,
    entry_bias,
    forget_rate,
    output_weight,
):
    hbm = pl.BlockSpec(memory_space=pltpu.HBM)
    return pl.pallas_call(
        kernel,
        name="layer",
        out_shape=pltpu.VMEM((SEQS, TOK, D), bf16),
        in_specs=[hbm] * 12,
        out_specs=pl.BlockSpec(memory_space=pltpu.VMEM),
        scratch_shapes=[
            pltpu.VMEM((1, D), f32),
            pltpu.VMEM((SEQS, STR, D), bf16),
            pltpu.VMEM((ROWS, D), bf16),
            pltpu.VMEM((NB, AROWS, W), bf16),
            pltpu.VMEM((NB, D, W), bf16),
            pltpu.VMEM((NB, W, D), bf16),
            pltpu.VMEM((NB, 8, 1, W), f32),
            pltpu.VMEM((NB, ROWS, W), f32),
            pltpu.VMEM((NB, 32, W), bf16),
            pltpu.VMEM((NB, 32, W), bf16),
            pltpu.VMEM((ROWS, CH), bf16),
            pltpu.VMEM((2, ROWS, W), f32),
            pltpu.VMEM((NB, ROWS, W), f32),
            pltpu.VMEM((NB, ROWS, W), f32),
            pltpu.VMEM((NB, ROWS, W), f32),
            pltpu.VMEM((NB, ROWS, W), f32),
            pltpu.VMEM((ROWS, CH), bf16),
            pltpu.VMEM((8, CH), bf16),
            pltpu.VMEM((4, 8, CH), bf16),
            pltpu.VMEM((8, CH), bf16),
            pltpu.VMEM((8, 8, CH), bf16),
            pltpu.VMEM((3, SEQS, TOK, D), bf16),
            pltpu.VMEM((2, 2, TOK, D), f32),
            pltpu.VMEM((2, 2, TOK, D), bf16),
            pltpu.VMEM((2, SEQS, TOK, D), bf16),
            pltpu.SemaphoreType.DMA((N_SENDS,)),
            pltpu.SemaphoreType.DMA((N_COPIES,)),
            pltpu.SemaphoreType.DMA((N_LOCAL,)),
        ],
        compiler_params=pltpu.CompilerParams(
            collective_id=0, has_side_effects=True, vmem_limit_bytes=VMEM_LIMIT
        ),
    )(
        tokens,
        norm_gain.reshape(1, D),
        entry_projection,
        valve_projection,
        recur_weight,
        entry_weight,
        filter_taps.reshape(4, 1, W),
        conv_bias.reshape(1, W),
        recur_bias.reshape(1, W),
        entry_bias.reshape(1, W),
        forget_rate.reshape(1, W),
        output_weight,
    )


def solution(mesh):
    fine = Mesh(mesh.devices.reshape(4, 2, 4, 4), ("x", "c", "z", "y"))
    SP, TP = ("x", "c"), ("z", "y")
    both = SP + TP
    placed = (
        P(None, both, None),
        P(),
        P(None, TP),
        P(None, TP),
        P(None, TP),
        P(TP),
        P(TP, None, None),
        P(TP),
        P(TP, None, None),
        P(TP),
        P(TP),
        P(TP, None),
    )
    return jax.shard_map(
        per_device, mesh=fine, in_specs=placed, out_specs=P(None, both, None), check_vma=False
    )
```

```python
import jax
import jax.numpy as jnp
from jax import lax
from jax.experimental import pallas as pl
from jax.experimental.pallas import tpu as pltpu
from jax.sharding import Mesh
from jax.sharding import PartitionSpec as P

MESH = pl.DeviceIdType.MESH
EPS = 1e-06
POWER = 8.0
TINY = 1e-37
SEQS = 4
TOK = 16
STR = 64
D = 2048
W = 128
NB = 4
CH = NB * W
ROWS = SEQS * STR
AROWS = D + 2 * W
PIECE = ((AROWS // 24, 0), (AROWS // 12, AROWS // 3), (D // 8, 0), (W // 8, 0))
f32 = jnp.float32
bf16 = jnp.bfloat16


class Slots:
    def __init__(self):
        self.index = {}

    def __call__(self, *key):
        return self.index.setdefault(key, len(self.index))


N_COPIES = 44
N_SENDS = 16
N_LOCAL = 6
VMEM_LIMIT = 66700000


def neg_expm1(t):
    s = 1.0 + t * (1.0 / 8.0)
    for n in (7.0, 6.0, 5.0, 4.0, 3.0, 2.0):
        s = 1.0 + t * (1.0 / n) * s
    return jnp.where(t > -0.5, -t * s, 1.0 - jnp.exp(t))


def sigmoid(v):
    return 1.0 / (1.0 + jnp.exp(-v))


def kernel(
    tok_ref,
    gain_ref,
    w1_ref,
    w2_ref,
    rw_ref,
    ew_ref,
    taps_ref,
    cb_ref,
    rb_ref,
    eb_ref,
    rate_ref,
    wo_ref,
    out_ref,
    gain,
    tr,
    nt,
    wa,
    wv,
    wog,
    sm,
    ci,
    hs,
    hr,
    cv,
    lg,
    de,
    pu,
    sg,
    gt,
    g16,
    s_own,
    l1,
    t_own,
    l2,
    pb,
    pf,
    rd,
    rb,
    ssem,
    rsem,
    lsem,
):
    X = lax.axis_index("x")
    C = lax.axis_index("c")
    Z = lax.axis_index("z")
    Y = lax.axis_index("y")
    g = X * 2 + C
    par = lax.rem(X, 2)

    def mod4(v):
        return lax.rem(v + 8, 4)

    def gdev(v):
        return {"x": v // 2, "c": lax.rem(v, 2)}

    nxt_z = mod4(Z + 1)
    nxt_g = lax.rem(g + jnp.where(Z == 3, 1, 0), 8)
    prv_z = mod4(Z - 1)
    prv_g = lax.rem(g + 8 - jnp.where(Z == 0, 1, 0), 8)
    nxt = {"x": nxt_g // 2, "c": lax.rem(nxt_g, 2), "z": nxt_z}
    prv = {"x": prv_g // 2, "c": lax.rem(prv_g, 2), "z": prv_z}
    yp, ym = {"y": mod4(Y + 1)}, {"y": mod4(Y - 1)}
    zp, zm = {"z": nxt_z}, {"z": prv_z}
    xp, xm = {"x": mod4(X + 1)}, {"x": mod4(X - 1)}
    mate = {"c": 1 - C}

    slot = Slots()
    local = Slots()
    scopes = []

    def mark(name):
        if scopes:
            scopes.pop().__exit__(None, None, None)
        if name:
            scopes.append(jax.named_scope(name))
            scopes[-1].__enter__()

    def remote(out, key, src, dst, dev):
        return pltpu.make_async_remote_copy(
            src_ref=src,
            dst_ref=dst,
            send_sem=ssem.at[out],
            recv_sem=rsem.at[slot(*key)],
            device_id=dev,
            device_id_type=MESH,
        )

    def send(out, key, src, dst, dev):
        remote(out, key, src, dst, dev).start()

    def arrived(key, dst):
        remote(0, key, dst, dst, mate).wait_recv()

    def left(out, ref):
        remote(out, ("t", 0, 0), ref, ref, mate).wait_send()

    def fetch(key, src, dst):
        copy = pltpu.make_async_copy(src, dst, lsem.at[local(key)])
        copy.start()
        return copy

    mark("own")
    own_tok = tr.at[:, pl.ds(pl.multiple_of(Y * TOK, TOK), TOK), :]
    c_tok = fetch("tok", tok_ref, own_tok)
    fetch("wa", w1_ref, wa.at[Z, pl.ds(0, D)])
    fetch("wa", rw_ref.at[0], wa.at[Z, pl.ds(D, W)])
    fetch("wa", ew_ref.at[0], wa.at[Z, pl.ds(D + W, W)])
    fetch("sm", taps_ref, sm.at[Z, pl.ds(0, 4)])
    for n, ref in enumerate((cb_ref, rb_ref, eb_ref, rate_ref)):
        fetch("sm", ref, sm.at[Z, 4 + n])
    c_gain = fetch("gain", gain_ref, gain)
    c_wv = fetch("w2", w2_ref, wv.at[Z])
    c_wo = fetch("wo", wo_ref, wog.at[Z])

    l2[...] = jnp.zeros_like(l2)

    mark("barrier")
    barrier = pltpu.get_barrier_semaphore()
    partners = [yp, ym] + [{"z": mod4(Z + d)} for d in (1, 2, 3)]
    partners += [gdev(lax.rem(g + d, 8)) for d in range(1, 8)] + [nxt, prv]
    for dev in partners:
        pl.semaphore_signal(barrier, inc=1, device_id=dev, device_id_type=MESH)
    pl.semaphore_wait(barrier, len(partners))

    mark("tokens")
    def tok(y, half):
        return tr.at[pl.ds(2 * half, 2), pl.ds(pl.multiple_of(y * TOK, TOK), TOK), :]

    y_m, y_p, y_d = mod4(Y - 1), mod4(Y + 1), mod4(Y + 2)
    c_tok.wait()
    send(0, ("t", 0, 0), tok(Y, 0), tok(Y, 0), yp)
    send(0, ("t", 1, 1), tok(Y, 1), tok(Y, 1), ym)
    send(0, ("t", 0, 1), tok(Y, 1), tok(Y, 1), yp)
    send(0, ("t", 1, 0), tok(Y, 0), tok(Y, 0), ym)

    def piece(m, z, q, core, h):
        rows, base = PIECE[m]
        k = core * 2 + h
        if m == 1:
            rows = 2 * rows
        else:
            k = k + q * 4
        place = pl.ds(pl.multiple_of(base + k * rows, 16), rows)
        if m == 3:
            return wog.at[z, place]
        return (wa, wa, wv)[m].at[z, place]

    blocks = (mod4(Z - 1), mod4(Z + 1), mod4(Z + 2))

    def own_piece(m, j, h):
        ref = piece(m, Z, par, C, h)
        send(1 + m, ("z", m, j == h), ref, ref, zm if j else zp)

    def own_first(m):
        own_piece(m, 0, 0)
        own_piece(m, 1, 1)

    def own_second(m):
        own_piece(m, 0, 1)
        own_piece(m, 1, 0)

    def both(m):
        return (wa, wa, wv, wog)[m].at[0, pl.ds(0, PIECE[m][0] * (4 if m == 1 else 2))]

    def z_pair(m, pair, key):
        arrived(("z", m, key), both(m))
        for j, h in pair:
            ref = piece(m, blocks[j], par, C, h)
            if (j, h) == (0, 0):
                send(1 + m, ("z", m, 2), ref, ref, zp)
            if (j, h) == (1, 1):
                send(1 + m, ("z", m, 2), ref, ref, zm)
        for j, h in pair:
            ref = piece(m, blocks[j], par, C, h)
            if m != 1:
                send(1 + m, ("x", m, key), ref, ref, xp if h == 0 else xm)
            send(1 + m, ("d", m), ref, ref, mate)

    def x_pair(m, pair, key):
        arrived(("x", m, key), both(m))
        for j, h in pair:
            ref = piece(m, blocks[j], 1 - par, C, h)
            send(1 + m, ("d", m), ref, ref, mate)

    NEAR, NEXT, FAR = ((0, 0), (1, 1)), ((0, 1), (1, 0)), ((2, 0), (2, 1))

    def near_z(m):
        z_pair(m, NEAR, True)

    def next_z(m):
        z_pair(m, NEXT, False)

    def far_z(m):
        z_pair(m, FAR, 2)

    def near_x(m):
        x_pair(m, NEAR, True)

    def next_x(m):
        x_pair(m, NEXT, False)

    def far_x(m):
        x_pair(m, FAR, 2)

    def volume(m, parts):
        return (wa, wa, wv, wog)[m].at[pl.ds(0, parts // 6), pl.ds(0, PIECE[m][0] * 6)]

    mark("weights")
    pltpu.make_async_copy(wa.at[0], wa.at[0], lsem.at[local("wa")]).wait()
    own_first(0)
    own_second(0)
    own_first(1)
    pltpu.make_async_copy(sm.at[0], sm.at[0], lsem.at[local("sm")]).wait()
    for d in (1, 2, 3):
        send(5, ("s",), sm.at[Z], sm.at[Z], {"z": mod4(Z + d)})

    def norm(y, half):
        rows = pl.ds(pl.multiple_of(y * TOK, TOK), TOK)
        v = tr[pl.ds(2 * half, 2), rows, :].astype(f32)
        v = v * lax.rsqrt(jnp.mean(v * v, axis=-1, keepdims=True) + EPS)
        v = (v * gain[...].reshape(1, 1, D)).astype(bf16)
        for s in range(2):
            nt[pl.ds(pl.multiple_of((2 * half + s) * STR + y * TOK, TOK), TOK), :] = v[s]

    mark("norm0")
    c_gain.wait()
    norm(Y, 0)
    norm(Y, 1)
    mark("net0")
    near_z(0)
    own_second(1)
    mark("net1")
    next_z(0)
    mark("net1t")
    arrived(("t", 0, 0), tok(y_m, 0))
    send(0, ("t", 2, 0), tok(y_m, 0), tok(y_m, 0), yp)
    arrived(("t", 1, 1), tok(y_p, 1))
    send(0, ("t", 2, 1), tok(y_p, 1), tok(y_p, 1), ym)
    mark("net2")
    near_z(1)
    c_wv.wait()
    own_first(2)
    own_second(2)
    c_wo.wait()
    own_first(3)
    own_second(3)
    mark("norm1")
    norm(y_m, 0)
    norm(y_p, 1)
    mark("net3")
    far_z(0)
    mark("net3a")
    near_x(0)
    next_x(0)
    mark("net3b")
    next_z(1)
    mark("net3t")
    arrived(("t", 0, 1), tok(y_m, 1))
    arrived(("t", 1, 0), tok(y_p, 0))
    mark("norm2")
    norm(y_m, 1)
    norm(y_p, 0)
    mark("net4")
    far_z(1)
    mark("net5")
    far_x(0)
    mark("net5t")
    arrived(("t", 2, 0), tok(y_d, 0))
    norm(y_d, 0)
    arrived(("t", 2, 1), tok(y_d, 1))
    norm(y_d, 1)
    mark("d0")
    arrived(("d", 0), volume(0, 12))
    arrived(("d", 1), volume(1, 12))

    mark("matmul1")

    def pair(ref, b):
        rhs = jnp.concatenate([ref[b, 0:D, :], ref[b + 1, 0:D, :]], axis=1)
        return jnp.dot(nt[...], rhs, preferred_element_type=f32).astype(bf16).astype(f32)

    for b in range(0, NB, 2):
        part = pair(wa, b)
        ci[b] = part[:, 0:W]
        ci[b + 1] = part[:, W : 2 * W]
        for n in (b, b + 1):
            for s in range(SEQS):
                last = part[s * STR + STR - 8 : s * STR + STR, (n - b) * W : (n - b + 1) * W]
                hs[n, s * 8 : s * 8 + 8, :] = last.astype(bf16)
    send(6, ("h",), hs, hr, nxt)
    mark("net6")
    near_z(2)
    arrived(("s",), sm.at[pl.ds(0, 3)])

    mark("conv")
    lane_row = lax.broadcasted_iota(jnp.int32, (8, W), 0)

    def convolve(b, at):
        acc = jnp.broadcast_to(sm[b, 4], (8, W))
        for k in range(4):
            acc = acc + at(k - 3) * sm[b, k]
        return acc

    for b in range(NB):
        for s in range(SEQS):
            x = [ci[b, pl.ds(s * STR + i, 8, stride=8), :] for i in range(8)]
            prev = {i - 8: pltpu.roll(x[i], 1, 0) for i in (5, 6, 7)}
            rows = []
            for i in range(8):
                rows.append(convolve(b, lambda n: x[i + n] if i + n >= 0 else prev[i + n]))
            cv[pl.ds(s * STR, STR), b * W : (b + 1) * W] = jnp.concatenate(rows, axis=0).astype(bf16)

    mark("gates")

    def gates(b, logit_r, logit_e, conv):
        r_gate = sigmoid(logit_r + sm[b, 5])
        e_gate = sigmoid(logit_e + sm[b, 6])
        log_decay = (-POWER * r_gate) * sm[b, 7]
        push = jnp.sqrt(neg_expm1(2.0 * log_decay)) * (e_gate * conv.astype(f32))
        return jnp.exp(log_decay), push

    def gate_dots(b, conv):
        return [
            jnp.dot(conv, wa[b, D + n * W : D + (n + 1) * W, :], preferred_element_type=f32)
            for n in range(2)
        ]

    for b in range(NB):
        cols = slice(b * W, (b + 1) * W)
        lg[0], lg[1] = gate_dots(b, cv[:, cols])
        for s in range(SEQS):
            rows = slice(s * STR, (s + 1) * STR)
            de[b, rows, :], pu[b, rows, :] = gates(b, lg[0, rows, :], lg[1, rows, :], cv[rows, cols])

    mark("net7")
    next_z(2)
    near_z(3)
    mark("halo")
    arrived(("h",), hr)
    mark("redo")
    start = jnp.logical_and(g == 0, Z == 0)
    for b in range(NB):
        tiles = []
        for s in range(SEQS):
            behind = jnp.where(start, 0.0, hr[b, s * 8 : s * 8 + 8, :].astype(f32))
            here = ci[b, s * STR : s * STR + 8, :]

            def at(n):
                if n == 0:
                    return here
                return jnp.where(lane_row < -n, pltpu.roll(behind, -n, 0), pltpu.roll(here, -n, 0))

            tiles.append(convolve(b, at))
        conv = jnp.concatenate(tiles, axis=0).astype(bf16)
        decay, push = gates(b, *gate_dots(b, conv), conv)
        for s in range(SEQS):
            chain = pl.ds(s * STR, 8, stride=8)
            de[b, chain, :] = decay[s * 8 : s * 8 + 8]
            pu[b, chain, :] = push[s * 8 : s * 8 + 8]

    mark("scan")
    ends = [[None] * SEQS for _ in range(NB)]
    for b in range(NB):
        cols = slice(b * W, (b + 1) * W)
        tot_a, tot_h = [], []
        for s in range(SEQS):
            a = de[b, s * STR : s * STR + 8, :]
            h = pu[b, s * STR : s * STR + 8, :]
            for i in range(1, 8):
                at = slice(s * STR + i * 8, s * STR + i * 8 + 8)
                step = de[b, at, :]
                h = step * h + pu[b, at, :]
                a = step * a
                de[b, at, :] = a
                pu[b, at, :] = h
            for n in (1, 2, 4):
                keep = lane_row >= n
                a_in = jnp.where(keep, pltpu.roll(a, n, 0), 1.0)
                h_in = jnp.where(keep, pltpu.roll(h, n, 0), 0.0)
                h = a * h_in + h
                a = a * a_in
            tot_a.append(a[7:8])
            tot_h.append(h[7:8])
            ends[b][s] = (
                jnp.where(lane_row >= 1, pltpu.roll(a, 1, 0), 1.0),
                jnp.where(lane_row >= 1, pltpu.roll(h, 1, 0), 0.0),
            )
        tot_a = [jnp.log(jnp.maximum(a, TINY)) for a in tot_a]
        s_own[:, cols] = jnp.concatenate(tot_a + tot_h, axis=0).astype(bf16)

    mark("states")
    for d in (2, 1, 3):
        send(7, ("e",), s_own, l1.at[Z], {"z": mod4(Z + d)})
    l1[Z] = s_own[...]
    near_x(2)
    next_z(3)
    far_z(2)
    next_x(2)
    near_x(3)
    far_z(3)
    mark("states1")
    arrived(("e",), l1.at[pl.ds(0, 3)])
    total_a, total_h = l1[0, 0:4].astype(f32), l1[0, 4:8].astype(f32)
    for k in range(1, 4):
        ka, kh = l1[k, 0:4].astype(f32), l1[k, 4:8].astype(f32)
        total_h = jnp.exp(ka) * total_h + kh
        total_a = ka + total_a
    t_own[...] = jnp.concatenate([total_a, total_h], axis=0).astype(bf16)

    def to_group(d):
        return remote(8 + d, ("g", d), t_own, l2.at[g], gdev(lax.rem(g + d, 8)))

    for d in (4, 5, 3, 2, 6, 7, 1):

        @pl.when(g + d < 8)
        def _():
            to_group(d).start()

    mark("net8")
    far_x(2)
    mark("net8d")
    arrived(("d", 2), volume(2, 12))
    mark("valve")
    for b in range(0, NB, 2):
        v = pair(wv, b)
        v = v / (1.0 + jnp.exp(-v))
        sg[b] = v[:, 0:W]
        sg[b + 1] = v[:, W : 2 * W]
    mark("net9")
    next_x(3)
    far_x(3)
    mark("states2")
    for d in range(1, 8):

        @pl.when(g - d >= 0)
        def _():
            arrived(("g", d), l2.at[lax.rem(g - d + 8, 8)])

    mark("entering")
    state = jnp.zeros((SEQS, CH), f32)
    for k in range(7):
        state = jnp.where(k < g, jnp.exp(l2[k, 0:4].astype(f32)) * state + l2[k, 4:8].astype(f32), state)
    for k in range(3):
        state = jnp.where(k < Z, jnp.exp(l1[k, 0:4].astype(f32)) * state + l1[k, 4:8].astype(f32), state)

    mark("gated")
    for b in range(NB):
        cols = slice(b * W, (b + 1) * W)
        for s in range(SEQS):
            chain_a, chain_h = ends[b][s]
            enter = chain_a * jnp.broadcast_to(state[s : s + 1, cols], (8, W)) + chain_h
            for i in range(8):
                at = s * STR + i * 8
                h = de[b, at : at + 8, :] * enter + pu[b, at : at + 8, :]
                places = pl.ds(s * STR + i, 8, stride=8)
                gt[b, places, :] = h * sg[b, places, :]
        g16[:, cols] = gt[b].astype(bf16)

    mark("d2")
    arrived(("d", 3), volume(3, 12))

    def product(y):
        lhs = jnp.concatenate(
            [g16[pl.ds(pl.multiple_of(s * STR + y * TOK, TOK), TOK), :] for s in range(SEQS)], axis=0
        )
        return jnp.dot(lhs, wog[...].reshape(CH, D), preferred_element_type=f32)

    mark("prod0")
    p = product(y_d).astype(bf16).reshape(SEQS, TOK, D)
    pb[0] = p
    send(8, ("r", 0), pb.at[0, pl.ds(0, 2)], rd.at[0], ym)
    send(8, ("r", 1), pb.at[0, pl.ds(2, 2)], rd.at[1], yp)
    mark("prod1")
    p = product(y_p).reshape(SEQS, TOK, D)
    pb[1, 0:2] = p[0:2].astype(bf16)
    send(8, ("r", 2), pb.at[1, pl.ds(0, 2)], rb.at[0, pl.ds(0, 2)], yp)
    pf[1] = p[2:4]
    p = product(y_m).reshape(SEQS, TOK, D)
    pb[2, 2:4] = p[2:4].astype(bf16)
    send(8, ("r", 2), pb.at[2, pl.ds(2, 2)], rb.at[1, pl.ds(2, 2)], ym)
    pf[0] = p[0:2]
    mine = product(Y).reshape(SEQS, TOK, D)
    mark("red1")
    arrived(("r", 1), rd.at[1])
    pb[1, 2:4] = (pf[1] + rd[1].astype(f32)).astype(bf16)
    send(8, ("r", 2), pb.at[1, pl.ds(2, 2)], rb.at[0, pl.ds(2, 2)], yp)
    arrived(("r", 0), rd.at[0])
    pb[2, 0:2] = (pf[0] + rd[0].astype(f32)).astype(bf16)
    send(8, ("r", 2), pb.at[2, pl.ds(0, 2)], rb.at[1, pl.ds(0, 2)], ym)
    mark("red2")
    arrived(("r", 2), rb)
    mark("final")
    out_ref[...] = (mine + rb[0].astype(f32) + rb[1].astype(f32)).astype(bf16)

    mark("drain")
    left(0, tr.at[pl.ds(0, 3)])
    for m in range(4):
        left(1 + m, volume(m, 24))
    left(5, sm.at[pl.ds(0, 3)])
    left(6, hs)
    left(7, l1.at[pl.ds(0, 3)])
    left(8, pb)
    for d in range(1, 8):

        @pl.when(g + d < 8)
        def _():
            to_group(d).wait_send()

    assert len(slot.index) == N_COPIES and len(local.index) == N_LOCAL
    mark(None)


def per_device(
    tokens,
    norm_gain,
    entry_projection,
    valve_projection,
    filter_taps,
    conv_bias,
    recur_weight,
    recur_bias,
    entry_weight,
    entry_bias,
    forget_rate,
    output_weight,
):
    hbm = pl.BlockSpec(memory_space=pltpu.HBM)
    return pl.pallas_call(
        kernel,
        name="layer",
        out_shape=pltpu.VMEM((SEQS, TOK, D), bf16),
        in_specs=[hbm] * 12,
        out_specs=pl.BlockSpec(memory_space=pltpu.VMEM),
        scratch_shapes=[
            pltpu.VMEM((1, D), f32),
            pltpu.VMEM((SEQS, STR, D), bf16),
            pltpu.VMEM((ROWS, D), bf16),
            pltpu.VMEM((NB, AROWS, W), bf16),
            pltpu.VMEM((NB, D, W), bf16),
            pltpu.VMEM((NB, W, D), bf16),
            pltpu.VMEM((NB, 8, 1, W), f32),
            pltpu.VMEM((NB, ROWS, W), f32),
            pltpu.VMEM((NB, 32, W), bf16),
            pltpu.VMEM((NB, 32, W), bf16),
            pltpu.VMEM((ROWS, CH), bf16),
            pltpu.VMEM((2, ROWS, W), f32),
            pltpu.VMEM((NB, ROWS, W), f32),
            pltpu.VMEM((NB, ROWS, W), f32),
            pltpu.VMEM((NB, ROWS, W), f32),
            pltpu.VMEM((NB, ROWS, W), f32),
            pltpu.VMEM((ROWS, CH), bf16),
            pltpu.VMEM((8, CH), bf16),
            pltpu.VMEM((4, 8, CH), bf16),
            pltpu.VMEM((8, CH), bf16),
            pltpu.VMEM((8, 8, CH), bf16),
            pltpu.VMEM((3, SEQS, TOK, D), bf16),
            pltpu.VMEM((2, 2, TOK, D), f32),
            pltpu.VMEM((2, 2, TOK, D), bf16),
            pltpu.VMEM((2, SEQS, TOK, D), bf16),
            pltpu.SemaphoreType.DMA((N_SENDS,)),
            pltpu.SemaphoreType.DMA((N_COPIES,)),
            pltpu.SemaphoreType.DMA((N_LOCAL,)),
        ],
        compiler_params=pltpu.CompilerParams(
            collective_id=0, has_side_effects=True, vmem_limit_bytes=VMEM_LIMIT
        ),
    )(
        tokens,
        norm_gain.reshape(1, D),
        entry_projection,
        valve_projection,
        recur_weight,
        entry_weight,
        filter_taps.reshape(4, 1, W),
        conv_bias.reshape(1, W),
        recur_bias.reshape(1, W),
        entry_bias.reshape(1, W),
        forget_rate.reshape(1, W),
        output_weight,
    )


def solution(mesh):
    fine = Mesh(mesh.devices.reshape(4, 2, 4, 4), ("x", "c", "z", "y"))
    SP, TP = ("x", "c"), ("z", "y")
    both = SP + TP
    placed = (
        P(None, both, None),
        P(),
        P(None, TP),
        P(None, TP),
        P(None, TP),
        P(TP),
        P(TP, None, None),
        P(TP),
        P(TP, None, None),
        P(TP),
        P(TP),
        P(TP, None),
    )
    return jax.shard_map(
        per_device, mesh=fine, in_specs=placed, out_specs=P(None, both, None), check_vma=False
    )
```
